32 devices in a mesh: sp: 16 (over z, y, x), tp: 2 (over core).
Axes of the slice: x: 2, y: 2, z: 4, core: 2. Of those that a mesh axis runs over, the one named last changes fastest.
Arguments:
- query: bfloat16 [2048, 2048], P('sp', 'tp'), may hold values from -6 to 6
- forget_logit: bfloat16 [2048, 2048], P('sp', 'tp'), may hold values from -7.5 to 7.5
- value: bfloat16 [2048, 2048], P('sp', 'tp'), may hold values from -6 to 6
- out_gate: bfloat16 [2048, 2048], P('sp', 'tp'), may hold values from -6 to 6
- lower_bound: float32 [2048], P('tp'), may hold values from 0.9 to 1, as said below
- head_gain: float32 [2048], P('tp'), may hold values from 0.1 to 1.9
- residual_in: bfloat16 [2048, 2048], P(('sp', 'tp')), may hold values from -6 to 6
- w_out: bfloat16 [2048, 2048], replicated, may hold values from -0.125 to 0.125
- ffn_gain: float32 [2048], replicated, may hold values from 0.1 to 1.9
- routing: int32 [2048, 2], P(('sp', 'tp')), may hold values from 0 to 15, all different within a row; in each aligned block of 64 rows (0 to 63, 64 to 127, ...) at most 16 rows name the same one
- route_weight: float32 [2048, 2], P(('sp', 'tp')), may hold values from 0.25 to 1
- expert_gate: bfloat16 [16, 2048, 1024], P('sp', None, 'tp'), may hold values from -0.125 to 0.125
- expert_up: bfloat16 [16, 2048, 1024], P('sp', None, 'tp'), may hold values from -0.125 to 0.125
- expert_down: bfloat16 [16, 1024, 2048], P('sp', 'tp'), may hold values from -0.1875 to 0.1875
Outputs:
- layer_out: bfloat16 [2048, 2048], P(('sp', 'tp'))
The draws below stay inside these ranges and needn't reach their ends.
Inputs may be any that keep to these rules, and one draw needn't show every extreme that they name: `routing`: each row names 2 different experts. In each aligned block of 64 rows (the rows of one device) no expert is named by more than 16 rows, a bound that some blocks reach. 1 - lower_bound is at least 1 / 4096.
All inputs are finite; a program needn't handle non-finite values.
Results may differ from the reference program's by a relative error of at most 0.012.
Values may be sent and summed in bfloat16 or wider, within the bound.
No kernel may reach another device: no remote copies, remote signals or barrier semaphores. Data moves between devices by JAX's collectives and lax.ppermute only.
A program may use at most 128 MiB of HBM per device.

```python
import math
import jax
import jax.numpy as jnp
import numpy as np
from jax import lax

D = 2048
HEADS = 16
HEAD_DIM = 128
FF = 1024
TOP_K = 2
BLOCK = 16
TOKENS = 2048
HALF = 64
EXPERTS = 16
CAP = 16
N_SP = 16
N_TP = 2


def draw_lower_bound(key, part):
    order_key, slow_key, fast_key, middle_key = jax.random.split(jax.random.fold_in(key, 11), 4)
    slow_count = HEADS // 2
    middle_count = max(1, HEADS // 5)
    ranks = jax.random.permutation(order_key, HEADS)
    middle_heads = ranks < middle_count
    slow_heads = ranks < slow_count
    slow_gap = jnp.exp(jax.random.uniform(slow_key, (HEADS, HEAD_DIM), jnp.float32, jnp.log(0.5), jnp.log(3.0))) / TOKENS
    fast_gap = jnp.exp(jax.random.uniform(fast_key, (HEADS, HEAD_DIM), jnp.float32, jnp.log(0.03), jnp.log(0.1)))
    middle_gap = jnp.exp(jax.random.uniform(middle_key, (HEADS, HEAD_DIM), jnp.float32, jnp.log(0.002), jnp.log(0.008)))
    gap_values = jnp.where(slow_heads[:, None], slow_gap, fast_gap)
    gap_values = jnp.where(middle_heads[:, None], middle_gap, gap_values)
    return (1.0 - gap_values).reshape(-1).astype(jnp.float32)


def draw_forget_logit(key, part):
    rough_key, span_key, wide_key = jax.random.split(jax.random.fold_in(key, 23), 3)
    width = HEADS * HEAD_DIM
    rows = jnp.arange(TOKENS)
    rough = jax.random.normal(rough_key, (TOKENS, width), jnp.float32)
    offsets = jax.random.uniform(span_key, (TOKENS // 128 + 1, width), jnp.float32, -1.5, 1.5)
    wide = jax.random.uniform(wide_key, (TOKENS // 1024 + 1, HEADS), jnp.float32, -1.5, 6.0)
    wide_full = jnp.repeat(wide, HEAD_DIM, axis=1)
    values = rough + offsets[rows // 128] + wide_full[rows // 1024]
    return jnp.clip(values, -7.5, 7.5).astype(jnp.bfloat16)


def block_scale(rng, extent, shards, low, top_value):
    loudness = 1.0
    for dim, parts in shards:
        steps = jax.random.uniform(jax.random.fold_in(jax.random.fold_in(rng, 6), dim), (parts,), jnp.float32, low / len(shards), top_value / len(shards))
        loudness = loudness * jnp.repeat(jnp.exp(steps), extent[dim] // parts).reshape((-1,) + (1,) * (len(extent) - 1 - dim))
    return loudness


def routed_block(key, own, number, rows, number_of, top, most, skew):
    order = jax.random.permutation(key, number_of)
    heavy_load, usual = load_shares(number_of, rows * top, most, skew, True), load_shares(number_of, rows * top, most, skew, False)
    places = jnp.arange(number_of)

    def named(sizes, rotation):
        used = int((sizes > 0).sum())
        fixed = max(1, used // 4)
        shifted = fixed + (places - fixed + rotation * (used - fixed)) % max(1, number_of - fixed)
        return jnp.zeros((number_of,), jnp.int32).at[order[jnp.where(places < fixed, places, shifted)]].set(jnp.asarray(sizes, jnp.int32))

    sizes = jnp.where(number % 4 == 0, named(heavy_load, number // 4), named(usual, number - number // 4 - 1))
    mixed = jax.random.permutation(jax.random.fold_in(own, 3), number_of)
    donor, taker = mixed[0:number_of // 2 * 2:2], mixed[1:number_of // 2 * 2:2]
    room = jnp.minimum(sizes[donor] - 1, most - sizes[taker]) // 2
    room = jnp.where((donor == order[0]) | (taker == order[0]) | (sizes[taker] == 0), 0, jnp.maximum(room, 0))
    shifted = jax.random.randint(jax.random.fold_in(own, 4), (number_of // 2,), 0, 1 << 20) % (room + 1)
    sizes = sizes.at[donor].add(-shifted).at[taker].add(shifted)
    labels = jnp.searchsorted(jnp.cumsum(sizes), jnp.arange(rows * top), side="right").astype(jnp.int32)
    table = labels.reshape(top, rows).T
    table = table[jax.random.permutation(jax.random.fold_in(own, 1), rows)]
    rotation = jax.random.randint(jax.random.fold_in(own, 2), (rows, 1), 0, top)
    return jnp.take_along_axis(table, (jnp.arange(top)[None, :] + rotation) % top, axis=1)


def load_shares(count, total, bound, slope, full):
    weights = [(1 << 20) // math.isqrt(rank ** slope) + 1 for rank in range(1, count + 1)]
    largest = bound if full else min(bound, max(-(-total // count), total * weights[0] // sum(weights)))
    least = 1 if total - largest >= count - 1 else 0
    holding, surplus = [largest] + [least] * (count - 1), total - largest - least * (count - 1)
    while surplus > 0:
        free = [i for i in range(1, count) if holding[i] < largest] or [i for i in range(1, count) if holding[i] < bound]
        pool, left = sum([weights[i] for i in free]), surplus
        for i in free:
            more = min(bound - holding[i], max(1, left * weights[i] // pool), surplus)
            holding[i] = holding[i] + more
            surplus = surplus - more
    return np.array(holding)


def scatter_about(stream_key, shape, deviation, bound, cuts=(), kind=jnp.bfloat16):
    values = deviation * jax.random.normal(stream_key, shape, jnp.float32)
    if cuts:
        values = values * block_scale(stream_key, shape, cuts, -0.22, 0.18)
    return jnp.clip(values, -bound, bound).astype(kind)


def setup_inputs(seed: int = 0) -> dict:
    arg_keys = jax.random.split(jax.random.key(seed), 15)
    query = scatter_about(arg_keys[0], (TOKENS, HEADS * HEAD_DIM), 1.0, 6.0, ((0, 16), (1, 2)))
    forget_logit = draw_forget_logit(jax.random.fold_in(arg_keys[14], 71), 0)
    value = scatter_about(arg_keys[2], (TOKENS, HEADS * HEAD_DIM), 1.0, 6.0, ((0, 16), (1, 2)))
    out_gate = scatter_about(arg_keys[3], (TOKENS, HEADS * HEAD_DIM), 1.0, 6.0, ((0, 16), (1, 2)))
    lower_bound = draw_lower_bound(jax.random.fold_in(arg_keys[14], 71), 0)
    head_gain = jnp.clip(1.0 + 0.18 * jax.random.normal(arg_keys[5], (HEADS * HEAD_DIM,), jnp.float32), 0.1, 1.9)
    residual_in = scatter_about(arg_keys[6], (TOKENS, D), 1.0, 6.0, ((0, 32),))
    w_out = scatter_about(arg_keys[7], (HEADS * HEAD_DIM, D), (HEADS * HEAD_DIM) ** -0.5, 0.125)
    ffn_gain = jnp.clip(1.0 + 0.18 * jax.random.normal(arg_keys[8], (D,), jnp.float32), 0.1, 1.9)
    routing_keys = jax.random.split(jax.random.fold_in(arg_keys[9], 1), TOKENS // HALF)
    routing_turns = jax.random.permutation(jax.random.fold_in(arg_keys[9], 3), TOKENS // HALF)
    routing = jax.vmap(lambda own, number: routed_block(jax.random.fold_in(arg_keys[9], 2), own, number, HALF, EXPERTS, TOP_K, CAP, 2))(routing_keys, routing_turns).reshape((TOKENS, TOP_K))
    route_weight = jnp.clip(0.25 + 0.75 * jax.random.uniform(arg_keys[10], (TOKENS, TOP_K), jnp.float32) ** block_scale(arg_keys[10], (TOKENS, TOP_K), ((0, 32),), -0.2, 0.2), 0.25, 1.0)
    expert_gate = scatter_about(arg_keys[11], (EXPERTS, D, FF), D ** -0.5, 0.125, ((0, 16), (2, 2)))
    expert_up = scatter_about(arg_keys[12], (EXPERTS, D, FF), D ** -0.5, 0.125, ((0, 16), (2, 2)))
    expert_down = scatter_about(arg_keys[13], (EXPERTS, FF, D), FF ** -0.5, 0.1875, ((0, 16), (1, 2)))
    return {"query": query, "forget_logit": forget_logit, "value": value, "out_gate": out_gate, "lower_bound": lower_bound, "head_gain": head_gain, "residual_in": residual_in, "w_out": w_out, "ffn_gain": ffn_gain, "routing": routing, "route_weight": route_weight, "expert_gate": expert_gate, "expert_up": expert_up, "expert_down": expert_down}


epsilon = 1e-06
highest = lax.Precision.HIGHEST

def recurrence(queries, log_forget, key_gate, values):
    blocks = queries.shape[0] // BLOCK

    def to_blocks(table):
        return table.reshape(blocks, BLOCK, HEADS, HEAD_DIM)
    causal = jnp.arange(BLOCK)[:, None] >= jnp.arange(BLOCK)[None, :]

    def advance(state, inputs):
        query_b, forget_b, key_b, value_b = inputs
        cumulative = jnp.cumsum(forget_b, axis=0)
        log_gaps = cumulative[:, None] - cumulative[None, :]
        decays = jnp.exp(jnp.where(causal[:, :, None, None], log_gaps, -jnp.inf))
        scores = jnp.einsum('thd,shd,tshd->hts', query_b, key_b, decays, precision=highest)
        result = jnp.einsum('hts,shv->thv', scores, value_b, precision=highest)
        result = result + jnp.einsum('thd,hdv->thv', query_b * jnp.exp(cumulative), state, precision=highest)
        last_log = cumulative[-1]
        weighted = key_b * jnp.exp(last_log[None] - cumulative)
        state = jnp.exp(last_log)[:, :, None] * state + jnp.einsum('shd,shv->hdv', weighted, value_b, precision=highest)
        return (state, result)
    initial = jnp.zeros((HEADS, HEAD_DIM, HEAD_DIM), jnp.float32)
    _, head_out = lax.scan(advance, initial, (to_blocks(queries), to_blocks(log_forget), to_blocks(key_gate), to_blocks(values)))
    return head_out.reshape(-1, HEADS, HEAD_DIM)

def expert_pass(normed, routing, route_weight, expert_gate, expert_up, expert_down):
    flat_routes = routing.reshape(-1)
    flat_weights = route_weight.reshape(-1)
    most_rows = N_SP * N_TP * CAP

    def visit(running, inputs):
        expert_id, gate_w, up_w, down_w = inputs
        matches = flat_routes == expert_id
        slots_found = jnp.nonzero(matches, size=most_rows, fill_value=0)[0]
        filled = jnp.arange(most_rows) < jnp.sum(matches)
        owners = slots_found // TOP_K
        taken = normed[owners]
        gate_part = jnp.dot(taken, gate_w, preferred_element_type=jnp.float32)
        up_part = jnp.dot(taken, up_w, preferred_element_type=jnp.float32)
        hidden = (jax.nn.silu(gate_part) * up_part).astype(jnp.bfloat16)
        expert_out = jnp.dot(hidden, down_w, preferred_element_type=jnp.float32).astype(jnp.bfloat16)
        scaled = jnp.where(filled, flat_weights[slots_found], 0.0)
        running = running.at[owners].add(expert_out.astype(jnp.float32) * scaled[:, None])
        return (running, None)
    initial = jnp.zeros(normed.shape, jnp.float32)
    expert_ids = jnp.arange(EXPERTS, dtype=jnp.int32)
    summed, _ = lax.scan(visit, initial, (expert_ids, expert_gate, expert_up, expert_down))
    return summed

def reference(query, forget_logit, value, out_gate, lower_bound, head_gain, residual_in, w_out, ffn_gain, routing, route_weight, expert_gate, expert_up, expert_down):
    positions = query.shape[0]
    grid = (positions, HEADS, HEAD_DIM)
    floor_gate = lower_bound.reshape(HEADS, HEAD_DIM)
    logits = forget_logit.astype(jnp.float32).reshape(grid)
    log_forget = jnp.logaddexp(jnp.log(floor_gate), jnp.log1p(-floor_gate) + jax.nn.log_sigmoid(logits))
    key_gate = (1.0 - floor_gate) * jax.nn.sigmoid(-logits)
    head_out = recurrence(query.astype(jnp.float32).reshape(grid), log_forget, key_gate, value.astype(jnp.float32).reshape(grid))
    normed_heads = head_out * lax.rsqrt(lax.optimization_barrier(jnp.mean(head_out * head_out, axis=-1, keepdims=True)) + epsilon)
    gates = jax.nn.silu(out_gate.astype(jnp.float32).reshape(grid))
    mixed = (normed_heads * head_gain.reshape(HEADS, HEAD_DIM) * gates).astype(jnp.bfloat16).reshape(positions, -1)
    projected = jnp.dot(mixed, w_out, preferred_element_type=jnp.float32)
    updated = (residual_in.astype(jnp.float32) + projected).astype(jnp.bfloat16)
    updated_f = updated.astype(jnp.float32)
    normed = (updated_f * lax.rsqrt(lax.optimization_barrier(jnp.mean(updated_f * updated_f, axis=-1, keepdims=True)) + epsilon) * ffn_gain).astype(jnp.bfloat16)
    expert_sum = expert_pass(normed, routing, route_weight, expert_gate, expert_up, expert_down)
    return (updated_f + expert_sum).astype(jnp.bfloat16)
```

```python
import functools

import jax
import jax.numpy as jnp
from jax import lax
from jax.experimental import pallas as pl
from jax.experimental.pallas import tpu as pltpu
from jax.sharding import PartitionSpec as P

HEAD_DIM = 128
TAIL = 8
epsilon = 1e-06
f32 = jnp.float32
bf16 = jnp.bfloat16

NN = (((1,), (0,)), ((), ()))
NT = (((1,), (1,)), ((), ()))
TN = (((0,), (0,)), ((), ()))


def dot(a, b, dims=NN):
    return lax.dot_general(a, b, dims, preferred_element_type=f32)


def split(x):
    hi = x.astype(bf16)
    return hi, (x - hi.astype(f32)).astype(bf16)


def sigmoid(x):
    return 1.0 / (1.0 + jnp.exp(-x))


def local_kernel(q_ref, f_ref, v_ref, low_ref, intra_ref, qe_ref, out_ref, *, heads, rows):
    length = q_ref.shape[0]
    per = HEAD_DIM // rows
    t = lax.broadcasted_iota(jnp.int32, (length, length), 0)
    s = lax.broadcasted_iota(jnp.int32, (length, length), 1)
    causal = t >= s
    tri = jnp.where(causal, 1.0, 0.0).astype(bf16)
    gap = 1.0 - low_ref[...]
    key_gate = gap * sigmoid(-f_ref[...].astype(f32))
    hi, lo = split(jnp.log1p(-key_gate))
    total = dot(tri, hi) + dot(tri, lo)
    middle = total[length // 2 - 1 : length // 2]
    last = total[length - 1 : length]
    query = q_ref[...].astype(f32)
    scaled_query = (query * jnp.exp(total - middle)).astype(bf16)
    scaled_key = (key_gate * jnp.exp(middle - total)).astype(bf16)
    weighted = (key_gate * jnp.exp(last - total)).astype(bf16)
    qe_ref[...] = (query * jnp.exp(total)).astype(bf16)
    last_hi, last_lo = split(last)
    place = lax.broadcasted_iota(jnp.int32, (TAIL, HEAD_DIM), 0)
    for h in range(heads):
        lanes = slice(h * HEAD_DIM, (h + 1) * HEAD_DIM)
        value = v_ref[:, lanes]
        scores = dot(scaled_query[:, lanes], scaled_key[:, lanes], NT)
        scores = jnp.where(causal, scores, 0.0).astype(bf16)
        intra_ref[:, lanes] = dot(scores, value)
        state = dot(value, weighted[:, lanes], TN).astype(bf16)
        tail = jnp.where(
            place == 0,
            last_hi[:, lanes].astype(f32),
            jnp.where(place == 1, last_lo[:, lanes].astype(f32), 0.0),
        ).astype(bf16)
        for j in range(per):
            out_ref[h * per + j, :rows] = state[j * rows : (j + 1) * rows]
            out_ref[h * per + j, rows:] = tail


def scan_kernel(in_ref, out_ref, *, rows):
    state = jnp.zeros((rows, HEAD_DIM), f32)
    for i in range(in_ref.shape[0]):
        out_ref[i] = state.astype(bf16)
        tail = in_ref[i, rows:].astype(f32)
        decay = jnp.exp(tail[0:1] + tail[1:2])
        state = state * decay + in_ref[i, :rows].astype(f32)


def mix_kernel(tp_ref, intra_ref, qe_ref, state_ref, gate_ref, gain_ref, mine_ref, send_ref, *, heads):
    half = mine_ref.shape[0]
    own = tp_ref[0]
    for ref, side in ((send_ref, 1 - own), (mine_ref, own)):
        at = pl.ds(pl.multiple_of(side * half, half), half)
        for h in range(heads):
            lanes = slice(h * HEAD_DIM, (h + 1) * HEAD_DIM)
            out = intra_ref[at, lanes] + dot(qe_ref[at, lanes], state_ref[h], NT)
            scale = lax.rsqrt(jnp.mean(out * out, axis=-1, keepdims=True) + epsilon)
            gate = gate_ref[at, lanes].astype(f32)
            ref[:, lanes] = (out * scale * gain_ref[:, lanes] * (gate * sigmoid(gate))).astype(bf16)


def slots_of(routing, capacity):
    count, top = routing.shape
    t = lax.broadcasted_iota(jnp.int32, (count, count), 0)
    s = lax.broadcasted_iota(jnp.int32, (count, count), 1)
    before = jnp.where(t > s, 1.0, 0.0).astype(bf16)
    lane = lax.broadcasted_iota(jnp.int32, (count, 128), 1)
    taken = jnp.zeros((1, 128), f32)
    slots = []
    for k in range(top):
        expert = routing[:, k : k + 1]
        named = jnp.where(lane == expert, 1.0, 0.0)
        rank = dot(before, named.astype(bf16)) + taken
        rank = jnp.sum(named * rank, axis=1, keepdims=True)
        slots.append(expert * capacity + rank.astype(jnp.int32))
        taken = taken + jnp.sum(named, axis=0, keepdims=True)
    return slots


def project_kernel(
    tp_ref, mine_ref, recv_ref, w_ref, res_ref, gain_ref, route_ref, upd_ref, box_ref, acc_ref, *, capacity
):
    step = pl.program_id(0)
    steps = pl.num_programs(0)

    @pl.when(step == 0)
    def _():
        acc_ref[...] = dot(mine_ref[...], w_ref[...])

    @pl.when((step > 0) & (step < steps // 2))
    def _():
        acc_ref[...] += dot(mine_ref[...], w_ref[...])

    @pl.when(step >= steps // 2)
    def _():
        acc_ref[...] += dot(recv_ref[...], w_ref[...])

    @pl.when(step == steps - 1)
    def _():
        updated = (res_ref[...].astype(f32) + acc_ref[...]).astype(bf16)
        upd_ref[...] = updated
        updated = updated.astype(f32)
        scale = lax.rsqrt(jnp.mean(updated * updated, axis=-1, keepdims=True) + epsilon)
        normed = (updated * scale * gain_ref[...]).astype(bf16)
        lane = lax.broadcasted_iota(jnp.int32, (normed.shape[0], box_ref.shape[0]), 1)
        chosen = jnp.zeros(lane.shape, f32)
        for slot in slots_of(route_ref[...], capacity):
            chosen = chosen + jnp.where(lane == slot, 1.0, 0.0)
        box_ref[...] = dot(chosen.astype(bf16), normed, TN).astype(bf16)


def expert_kernel(x_ref, g0_ref, u0_ref, d0_ref, g1_ref, u1_ref, d1_ref, out_ref, acc_ref):
    step = pl.program_id(0)
    steps = pl.num_programs(0)

    def part(g_ref, u_ref, d_ref):
        x = x_ref[...]
        gate = dot(x, g_ref[...])
        hidden = (gate * sigmoid(gate) * dot(x, u_ref[...])).astype(bf16)
        return dot(hidden, d_ref[...])

    @pl.when(step == 0)
    def _():
        acc_ref[...] = part(g0_ref, u0_ref, d0_ref)

    @pl.when((step > 0) & (step < steps // 2))
    def _():
        acc_ref[...] += part(g0_ref, u0_ref, d0_ref)

    @pl.when(step >= steps // 2)
    def _():
        acc_ref[...] += part(g1_ref, u1_ref, d1_ref)

    @pl.when(step == steps - 1)
    def _():
        out_ref[...] = acc_ref[...].astype(bf16)


def combine_kernel(route_ref, weight_ref, back_ref, upd_ref, out_ref, *, capacity):
    lane = lax.broadcasted_iota(jnp.int32, (upd_ref.shape[0], back_ref.shape[0]), 1)
    chosen = jnp.zeros(lane.shape, f32)
    for k, slot in enumerate(slots_of(route_ref[...], capacity)):
        chosen = chosen + jnp.where(lane == slot, weight_ref[:, k : k + 1], 0.0)
    hi, lo = split(chosen)
    back = back_ref[...]
    out_ref[...] = (upd_ref[...].astype(f32) + (dot(hi, back) + dot(lo, back))).astype(bf16)


def params(mib, dims=1):
    return pltpu.CompilerParams(
        dimension_semantics=("arbitrary",) * dims, vmem_limit_bytes=mib * 1024 * 1024
    )


def body(
    query,
    forget_logit,
    value,
    out_gate,
    lower_bound,
    head_gain,
    residual_in,
    w_out,
    ffn_gain,
    routing,
    route_weight,
    expert_gate,
    expert_up,
    expert_down,
):
    ranks = lax.axis_size("sp")
    sides = lax.axis_size("tp")
    length, channels = query.shape
    heads = channels // HEAD_DIM
    rows = channels // ranks
    half = length // sides
    width = w_out.shape[1]
    top = routing.shape[1]
    capacity = 2 * half * top // ranks
    slots = ranks * capacity
    units = expert_gate.shape[2]
    tp = lax.axis_index("tp").reshape(1)
    swap = [(i, i ^ 1) for i in range(sides)]

    weights = (expert_gate[0], expert_up[0], expert_down[0])
    others = tuple(lax.ppermute(w, "tp", swap) for w in weights)

    group = 2
    intra, qe, packed = pl.pallas_call(
        functools.partial(local_kernel, heads=group, rows=rows),
        grid=(heads // group,),
        in_specs=[
            pl.BlockSpec((length, group * HEAD_DIM), lambda i: (0, i)),
            pl.BlockSpec((length, group * HEAD_DIM), lambda i: (0, i)),
            pl.BlockSpec((length, group * HEAD_DIM), lambda i: (0, i)),
            pl.BlockSpec((1, group * HEAD_DIM), lambda i: (0, i)),
        ],
        out_specs=[
            pl.BlockSpec((length, group * HEAD_DIM), lambda i: (0, i)),
            pl.BlockSpec((length, group * HEAD_DIM), lambda i: (0, i)),
            pl.BlockSpec((group * HEAD_DIM // rows, rows + TAIL, HEAD_DIM), lambda i: (i, 0, 0)),
        ],
        out_shape=[
            jax.ShapeDtypeStruct((length, channels), f32),
            jax.ShapeDtypeStruct((length, channels), bf16),
            jax.ShapeDtypeStruct((ranks, rows + TAIL, HEAD_DIM), bf16),
        ],
        compiler_params=params(16),
        name="local",
    )(query, forget_logit, value, lower_bound.reshape(1, -1))

    gathered = lax.all_to_all(packed, "sp", split_axis=0, concat_axis=0, tiled=True)
    prior = pl.pallas_call(
        functools.partial(scan_kernel, rows=rows),
        out_shape=jax.ShapeDtypeStruct((ranks, rows, HEAD_DIM), bf16),
        compiler_params=params(16, 0),
        name="scan",
    )(gathered)
    carried = lax.all_to_all(prior, "sp", split_axis=0, concat_axis=0, tiled=True)

    mine, send = pl.pallas_call(
        functools.partial(mix_kernel, heads=heads),
        grid_spec=pltpu.PrefetchScalarGridSpec(
            num_scalar_prefetch=1,
            grid=(1,),
            in_specs=[
                pl.BlockSpec((length, channels), lambda i, t: (0, 0)),
                pl.BlockSpec((length, channels), lambda i, t: (0, 0)),
                pl.BlockSpec((heads, HEAD_DIM, HEAD_DIM), lambda i, t: (0, 0, 0)),
                pl.BlockSpec((length, channels), lambda i, t: (0, 0)),
                pl.BlockSpec((1, channels), lambda i, t: (0, 0)),
            ],
            out_specs=[pl.BlockSpec((half, channels), lambda i, t: (0, 0))] * 2,
        ),
        out_shape=[jax.ShapeDtypeStruct((half, channels), bf16)] * 2,
        compiler_params=params(16),
        name="mix",
    )(tp, intra, qe, carried.reshape(heads, HEAD_DIM, HEAD_DIM), out_gate, head_gain.reshape(1, -1))
    recv = lax.ppermute(send, "tp", swap)

    block = 256
    per = channels // block
    updated, outbox = pl.pallas_call(
        functools.partial(project_kernel, capacity=capacity),
        grid_spec=pltpu.PrefetchScalarGridSpec(
            num_scalar_prefetch=1,
            grid=(sides * per,),
            in_specs=[
                pl.BlockSpec((half, block), lambda i, t: (0, jnp.minimum(i, per - 1))),
                pl.BlockSpec((half, block), lambda i, t: (0, jnp.maximum(i - per, 0))),
                pl.BlockSpec((block, width), lambda i, t: ((t[0] ^ (i // per)) * per + i % per, 0)),
                pl.BlockSpec((half, width), lambda i, t: (0, 0)),
                pl.BlockSpec((1, width), lambda i, t: (0, 0)),
                pl.BlockSpec((half, top), lambda i, t: (0, 0)),
            ],
            out_specs=[
                pl.BlockSpec((half, width), lambda i, t: (0, 0)),
                pl.BlockSpec((slots, width), lambda i, t: (0, 0)),
            ],
            scratch_shapes=[pltpu.VMEM((half, width), f32)],
        ),
        out_shape=[
            jax.ShapeDtypeStruct((half, width), bf16),
            jax.ShapeDtypeStruct((slots, width), bf16),
        ],
        compiler_params=params(24),
        name="project",
    )(tp, mine, recv, w_out, residual_in, ffn_gain.reshape(1, -1), routing)

    arrived = lax.all_to_all(
        outbox.reshape(ranks, capacity, width), "sp", split_axis=0, concat_axis=0, tiled=True
    )

    unit = 256
    parts = units // unit

    def first(i):
        return jnp.minimum(i, parts - 1)

    def second(i):
        return jnp.maximum(i - parts, 0)

    expert_out = pl.pallas_call(
        expert_kernel,
        grid=(2 * parts,),
        in_specs=[
            pl.BlockSpec((slots, width), lambda i: (0, 0)),
            pl.BlockSpec((width, unit), lambda i: (0, first(i))),
            pl.BlockSpec((width, unit), lambda i: (0, first(i))),
            pl.BlockSpec((unit, width), lambda i: (first(i), 0)),
            pl.BlockSpec((width, unit), lambda i: (0, second(i))),
            pl.BlockSpec((width, unit), lambda i: (0, second(i))),
            pl.BlockSpec((unit, width), lambda i: (second(i), 0)),
        ],
        out_specs=pl.BlockSpec((slots, width), lambda i: (0, 0)),
        out_shape=jax.ShapeDtypeStruct((slots, width), bf16),
        scratch_shapes=[pltpu.VMEM((slots, width), f32)],
        compiler_params=params(32),
        name="experts",
    )(arrived.reshape(slots, width), *weights, *others)

    returned = lax.all_to_all(
        expert_out.reshape(ranks, capacity, width), "sp", split_axis=0, concat_axis=0, tiled=True
    )
    columns = width // 4
    return pl.pallas_call(
        functools.partial(combine_kernel, capacity=capacity),
        grid=(width // columns,),
        in_specs=[
            pl.BlockSpec((half, top), lambda i: (0, 0)),
            pl.BlockSpec((half, top), lambda i: (0, 0)),
            pl.BlockSpec((slots, columns), lambda i: (0, i)),
            pl.BlockSpec((half, columns), lambda i: (0, i)),
        ],
        out_specs=pl.BlockSpec((half, columns), lambda i: (0, i)),
        out_shape=jax.ShapeDtypeStruct((half, width), bf16),
        compiler_params=params(16),
        name="combine",
    )(routing, route_weight, returned.reshape(slots, width), updated)


def solution(mesh):
    placed = (
        P("sp", "tp"),
        P("sp", "tp"),
        P("sp", "tp"),
        P("sp", "tp"),
        P("tp"),
        P("tp"),
        P(("sp", "tp"), None),
        P(),
        P(),
        P(("sp", "tp"), None),
        P(("sp", "tp"), None),
        P("sp", None, "tp"),
        P("sp", None, "tp"),
        P("sp", "tp", None),
    )
    return jax.shard_map(
        body, mesh=mesh, in_specs=placed, out_specs=P(("sp", "tp"), None), check_vma=False
    )
```

```python
import functools

import jax
import jax.numpy as jnp
from jax import lax
from jax.experimental import pallas as pl
from jax.experimental.pallas import tpu as pltpu
from jax.sharding import PartitionSpec as P

HEAD_DIM = 128
TAIL = 8
GROUPS = 4
COLUMNS = 4
epsilon = 1e-06
f32 = jnp.float32
bf16 = jnp.bfloat16

NN = (((1,), (0,)), ((), ()))
NT = (((1,), (1,)), ((), ()))
TN = (((0,), (0,)), ((), ()))


def dot(a, b, dims=NN):
    return lax.dot_general(a, b, dims, preferred_element_type=f32)


def split(x):
    hi = x.astype(bf16)
    return hi, (x - hi.astype(f32)).astype(bf16)


def sigmoid(x):
    return 1.0 / (1.0 + jnp.exp(-x))


def fetch(copies):
    for copy in copies:
        copy.start()
    return copies


def local_kernel(
    q_hbm, f_hbm, v_hbm, low_hbm, intra_ref, qe_ref, out_ref, q_ref, f_ref, v_ref, low_ref, sem, *, rows
):
    length, channels = q_ref.shape
    per = HEAD_DIM // rows
    block = channels // GROUPS
    low = pltpu.make_async_copy(low_hbm, low_ref, sem.at[3 * GROUPS])
    low.start()
    copies = []
    for g in range(GROUPS):
        lanes = slice(g * block, (g + 1) * block)
        copies.append(
            fetch(
                [
                    pltpu.make_async_copy(hbm.at[:, lanes], ref.at[:, lanes], sem.at[3 * g + i])
                    for i, (hbm, ref) in enumerate(((f_hbm, f_ref), (q_hbm, q_ref), (v_hbm, v_ref)))
                ]
            )
        )
    t = lax.broadcasted_iota(jnp.int32, (length, length), 0)
    s = lax.broadcasted_iota(jnp.int32, (length, length), 1)
    causal = t >= s
    tri = jnp.where(causal, 1.0, 0.0).astype(bf16)
    place = lax.broadcasted_iota(jnp.int32, (TAIL, HEAD_DIM), 0)
    low.wait()
    for g in range(GROUPS):
        group = slice(g * block, (g + 1) * block)
        for copy in copies[g]:
            copy.wait()
        gap = 1.0 - low_ref[:, group]
        key_gate = gap * sigmoid(-f_ref[:, group].astype(f32))
        hi, lo = split(jnp.log1p(-key_gate))
        total = dot(tri, hi) + dot(tri, lo)
        middle = total[length // 2 - 1 : length // 2]
        last = total[length - 1 : length]
        query = q_ref[:, group].astype(f32)
        scaled_query = (query * jnp.exp(total - middle)).astype(bf16)
        scaled_key = (key_gate * jnp.exp(middle - total)).astype(bf16)
        weighted = (key_gate * jnp.exp(last - total)).astype(bf16)
        qe_ref[:, group] = (query * jnp.exp(total)).astype(bf16)
        last_hi, last_lo = split(last)
        for i in range(block // HEAD_DIM):
            h = g * (block // HEAD_DIM) + i
            inner = slice(i * HEAD_DIM, (i + 1) * HEAD_DIM)
            lanes = slice(h * HEAD_DIM, (h + 1) * HEAD_DIM)
            value = v_ref[:, lanes]
            state = dot(value, weighted[:, inner], TN).astype(bf16)
            scores = dot(scaled_query[:, inner], scaled_key[:, inner], NT)
            scores = jnp.where(causal, scores, 0.0).astype(bf16)
            intra_ref[:, lanes] = dot(scores, value)
            tail = jnp.where(
                place == 0,
                last_hi[:, inner].astype(f32),
                jnp.where(place == 1, last_lo[:, inner].astype(f32), 0.0),
            ).astype(bf16)
            for j in range(per):
                out_ref[h * per + j, :rows] = state[j * rows : (j + 1) * rows]
                out_ref[h * per + j, rows:] = tail


def scan_kernel(in_ref, out_ref, *, rows):
    state = jnp.zeros((rows, HEAD_DIM), f32)
    for i in range(in_ref.shape[0]):
        out_ref[i] = state.astype(bf16)
        tail = in_ref[i, rows:].astype(f32)
        decay = jnp.exp(tail[0:1] + tail[1:2])
        state = state * decay + in_ref[i, :rows].astype(f32)


def mixed_head(h, at, intra_ref, qe_ref, state_ref, gate_ref, gain_ref):
    lanes = slice(h * HEAD_DIM, (h + 1) * HEAD_DIM)
    out = intra_ref[at, lanes] + dot(qe_ref[at, lanes], state_ref[h], NT)
    scale = lax.rsqrt(jnp.mean(out * out, axis=-1, keepdims=True) + epsilon)
    gate = gate_ref[:, lanes].astype(f32)
    return (out * scale * gain_ref[:, lanes] * (gate * sigmoid(gate))).astype(bf16)


def send_kernel(tp_ref, intra_ref, qe_ref, state_ref, gate_hbm, gain_hbm, send_ref, gate_ref, gain_ref, sem):
    half = send_ref.shape[0]
    at = pl.ds(pl.multiple_of((1 - tp_ref[0]) * half, half), half)
    copies = fetch(
        [
            pltpu.make_async_copy(gate_hbm.at[at], gate_ref, sem.at[0]),
            pltpu.make_async_copy(gain_hbm, gain_ref, sem.at[1]),
        ]
    )
    for copy in copies:
        copy.wait()
    for h in range(state_ref.shape[0]):
        lanes = slice(h * HEAD_DIM, (h + 1) * HEAD_DIM)
        send_ref[:, lanes] = mixed_head(h, at, intra_ref, qe_ref, state_ref, gate_ref, gain_ref)


def keep_kernel(
    tp_ref, intra_ref, qe_ref, state_ref, gate_hbm, gain_hbm, w_hbm, acc_ref, gate_ref, gain_ref, mix_ref, w_ref, sem
):
    half, width = acc_ref.shape
    channels = mix_ref.shape[1]
    own = tp_ref[0]
    at = pl.ds(pl.multiple_of(own * half, half), half)
    copies = fetch(
        [
            pltpu.make_async_copy(gate_hbm.at[at], gate_ref, sem.at[0]),
            pltpu.make_async_copy(gain_hbm, gain_ref, sem.at[1]),
        ]
    )
    block = width // COLUMNS
    from_row = pl.ds(pl.multiple_of(own * channels, channels), channels)
    weights = fetch(
        [
            pltpu.make_async_copy(
                w_hbm.at[from_row, n * block : (n + 1) * block],
                w_ref.at[:, n * block : (n + 1) * block],
                sem.at[2 + n],
            )
            for n in range(COLUMNS)
        ]
    )
    for copy in copies:
        copy.wait()
    for h in range(state_ref.shape[0]):
        lanes = slice(h * HEAD_DIM, (h + 1) * HEAD_DIM)
        mix_ref[:, lanes] = mixed_head(h, at, intra_ref, qe_ref, state_ref, gate_ref, gain_ref)
    for n in range(COLUMNS):
        weights[n].wait()
        lanes = slice(n * block, (n + 1) * block)
        acc_ref[:, lanes] = dot(mix_ref[...], w_ref[:, lanes])


def slots_of(routing, capacity):
    count, top = routing.shape
    t = lax.broadcasted_iota(jnp.int32, (count, count), 0)
    s = lax.broadcasted_iota(jnp.int32, (count, count), 1)
    before = jnp.where(t > s, 1.0, 0.0).astype(bf16)
    lane = lax.broadcasted_iota(jnp.int32, (count, 128), 1)
    taken = jnp.zeros((1, 128), f32)
    slots = []
    for k in range(top):
        expert = routing[:, k : k + 1]
        named = jnp.where(lane == expert, 1.0, 0.0)
        rank = dot(before, named.astype(bf16)) + taken
        rank = jnp.sum(named * rank, axis=1, keepdims=True)
        slots.append(expert * capacity + rank.astype(jnp.int32))
        taken = taken + jnp.sum(named, axis=0, keepdims=True)
    return slots


def project_kernel(
    tp_ref, recv_ref, acc_ref, route_ref, w_hbm, res_hbm, gain_hbm, upd_ref, box_hbm,
    w_ref, res_ref, gain_ref, box_ref, sem, *, capacity,
):
    half, width = acc_ref.shape
    channels = recv_ref.shape[1]
    other = 1 - tp_ref[0]
    block = width // COLUMNS
    from_row = pl.ds(pl.multiple_of(other * channels, channels), channels)
    weights = fetch(
        [
            pltpu.make_async_copy(
                w_hbm.at[from_row, n * block : (n + 1) * block],
                w_ref.at[:, n * block : (n + 1) * block],
                sem.at[2 + n],
            )
            for n in range(COLUMNS)
        ]
    )
    copies = fetch(
        [
            pltpu.make_async_copy(res_hbm, res_ref, sem.at[0]),
            pltpu.make_async_copy(gain_hbm, gain_ref, sem.at[1]),
        ]
    )
    lane = lax.broadcasted_iota(jnp.int32, (half, box_ref.shape[0]), 1)
    chosen = jnp.zeros(lane.shape, f32)
    for slot in slots_of(route_ref[...], capacity):
        chosen = chosen + jnp.where(lane == slot, 1.0, 0.0)
    chosen = chosen.astype(bf16)
    square = jnp.zeros((half, 1), f32)
    recv = recv_ref[...]
    for n in range(COLUMNS):
        lanes = slice(n * block, (n + 1) * block)
        weights[n].wait()
        if n == 0:
            for copy in copies:
                copy.wait()
        updated = (res_ref[:, lanes].astype(f32) + (acc_ref[:, lanes] + dot(recv, w_ref[:, lanes]))).astype(bf16)
        upd_ref[:, lanes] = updated
        updated = updated.astype(f32)
        square = square + jnp.sum(updated * updated, axis=-1, keepdims=True)
    scale = lax.rsqrt(square * (1.0 / width) + epsilon)
    stores = []
    for n in range(COLUMNS):
        lanes = slice(n * block, (n + 1) * block)
        normed = (upd_ref[:, lanes].astype(f32) * scale * gain_ref[:, lanes]).astype(bf16)
        box_ref[:, lanes] = dot(chosen, normed, TN).astype(bf16)
        stores.append(
            pltpu.make_async_copy(box_ref.at[:, lanes], box_hbm.at[:, lanes], sem.at[2 + COLUMNS + n])
        )
        stores[n].start()
    for copy in stores:
        copy.wait()


def expert_kernel(
    x_ref, g0_hbm, u0_hbm, d0_hbm, g1_hbm, u1_hbm, d1_hbm, out_hbm, g_ref, u_ref, d_ref, hid_ref, out_ref, sem
):
    units = g0_hbm.shape[1]
    width = d0_hbm.shape[1]
    block = 256
    parts = units // block
    ups = []
    for side, (g_hbm, u_hbm) in enumerate(((g0_hbm, u0_hbm), (g1_hbm, u1_hbm))):
        for j in range(parts):
            i = side * parts + j
            here = slice(j * block, (j + 1) * block)
            there = slice(i * block, (i + 1) * block)
            ups.append(
                fetch(
                    [
                        pltpu.make_async_copy(g_hbm.at[:, here], g_ref.at[:, there], sem.at[2 * i]),
                        pltpu.make_async_copy(u_hbm.at[:, here], u_ref.at[:, there], sem.at[2 * i + 1]),
                    ]
                )
            )
    base = 4 * parts
    downs = fetch(
        [
            pltpu.make_async_copy(d0_hbm, d_ref.at[:units], sem.at[base]),
            pltpu.make_async_copy(d1_hbm, d_ref.at[units:], sem.at[base + 1]),
        ]
    )
    x = x_ref[...]
    for i in range(2 * parts):
        lanes = slice(i * block, (i + 1) * block)
        for copy in ups[i]:
            copy.wait()
        gate = dot(x, g_ref[:, lanes])
        hid_ref[:, lanes] = (gate * sigmoid(gate) * dot(x, u_ref[:, lanes])).astype(bf16)
    for copy in downs:
        copy.wait()
    block = width // COLUMNS
    stores = []
    for n in range(COLUMNS):
        lanes = slice(n * block, (n + 1) * block)
        out_ref[:, lanes] = dot(hid_ref[...], d_ref[:, lanes]).astype(bf16)
        stores.append(pltpu.make_async_copy(out_ref.at[:, lanes], out_hbm.at[:, lanes], sem.at[base + 2 + n]))
        stores[n].start()
    for copy in stores:
        copy.wait()


def combine_kernel(route_ref, weight_ref, back_ref, upd_ref, out_ref, *, capacity):
    lane = lax.broadcasted_iota(jnp.int32, (upd_ref.shape[0], back_ref.shape[0]), 1)
    chosen = jnp.zeros(lane.shape, f32)
    for k, slot in enumerate(slots_of(route_ref[...], capacity)):
        chosen = chosen + jnp.where(lane == slot, weight_ref[:, k : k + 1], 0.0)
    hi, lo = split(chosen)
    back = back_ref[...]
    out_ref[...] = (upd_ref[...].astype(f32) + (dot(hi, back) + dot(lo, back))).astype(bf16)


HBM = pl.BlockSpec(memory_space=pltpu.HBM)
SMEM = pl.BlockSpec(memory_space=pltpu.SMEM)
VMEM = pl.BlockSpec(memory_space=pltpu.VMEM)


def call(kernel, name, ins, outs, scratch=(), mib=16):
    run = pl.pallas_call(
        kernel,
        in_specs=ins,
        out_specs=[spec for spec, _ in outs],
        out_shape=[
            pltpu.HBM(shape.shape, shape.dtype) if spec is HBM else shape for spec, shape in outs
        ],
        scratch_shapes=list(scratch),
        compiler_params=pltpu.CompilerParams(vmem_limit_bytes=mib * 1024 * 1024),
        name=name,
    )

    def placed(*args):
        return run(
            *(
                pltpu.with_memory_space_constraint(arg, pltpu.HBM) if spec is HBM else arg
                for spec, arg in zip(ins, args)
            )
        )

    return placed


def body(
    query,
    forget_logit,
    value,
    out_gate,
    lower_bound,
    head_gain,
    residual_in,
    w_out,
    ffn_gain,
    routing,
    route_weight,
    expert_gate,
    expert_up,
    expert_down,
):
    shape = jax.ShapeDtypeStruct
    dma = pltpu.SemaphoreType.DMA
    ranks = lax.axis_size("sp")
    sides = lax.axis_size("tp")
    length, channels = query.shape
    heads = channels // HEAD_DIM
    rows = channels // ranks
    half = length // sides
    width = w_out.shape[1]
    top = routing.shape[1]
    capacity = 2 * half * top // ranks
    slots = ranks * capacity
    units = expert_gate.shape[2]
    tp = lax.axis_index("tp").reshape(1)
    swap = [(i, i ^ 1) for i in range(sides)]

    weights = (expert_gate[0], expert_up[0], expert_down[0])
    others = tuple(lax.ppermute(w, "tp", swap) for w in weights)

    intra, qe, packed = call(
        functools.partial(local_kernel, rows=rows),
        "local",
        [HBM] * 4,
        [
            (VMEM, shape((length, channels), f32)),
            (VMEM, shape((length, channels), bf16)),
            (VMEM, shape((ranks, rows + TAIL, HEAD_DIM), bf16)),
        ],
        [pltpu.VMEM((length, channels), bf16)] * 3
        + [pltpu.VMEM((1, channels), f32), dma((3 * GROUPS + 1,))],
    )(query, forget_logit, value, lower_bound.reshape(1, -1))

    gathered = lax.all_to_all(packed, "sp", split_axis=0, concat_axis=0, tiled=True)
    (prior,) = call(
        functools.partial(scan_kernel, rows=rows),
        "scan",
        [VMEM],
        [(VMEM, shape((ranks, rows, HEAD_DIM), bf16))],
    )(gathered)
    carried = lax.all_to_all(prior, "sp", split_axis=0, concat_axis=0, tiled=True)

    mix_args = (
        tp,
        intra,
        qe,
        carried.reshape(heads, HEAD_DIM, HEAD_DIM),
        out_gate,
        head_gain.reshape(1, -1),
    )
    mix_specs = [SMEM, VMEM, VMEM, VMEM, HBM, HBM]
    mix_scratch = [pltpu.VMEM((half, channels), bf16), pltpu.VMEM((1, channels), f32)]
    (send,) = call(
        send_kernel,
        "send",
        mix_specs,
        [(VMEM, shape((half, channels), bf16))],
        mix_scratch + [dma((2,))],
    )(*mix_args)
    recv = lax.ppermute(send, "tp", swap)
    (partial,) = call(
        keep_kernel,
        "keep",
        mix_specs + [HBM],
        [(VMEM, shape((half, width), f32))],
        mix_scratch
        + [pltpu.VMEM((half, channels), bf16), pltpu.VMEM((channels, width), bf16), dma((2 + COLUMNS,))],
    )(*mix_args, w_out)
    updated, outbox = call(
        functools.partial(project_kernel, capacity=capacity),
        "project",
        [SMEM, VMEM, VMEM, VMEM, HBM, HBM, HBM],
        [(VMEM, shape((half, width), bf16)), (HBM, shape((slots, width), bf16))],
        [
            pltpu.VMEM((channels, width), bf16),
            pltpu.VMEM((half, width), bf16),
            pltpu.VMEM((1, width), f32),
            pltpu.VMEM((slots, width), bf16),
            dma((2 + 2 * COLUMNS,)),
        ],
    )(tp, recv, partial, routing, w_out, residual_in, ffn_gain.reshape(1, -1))

    arrived = lax.all_to_all(
        outbox.reshape(ranks, capacity, width), "sp", split_axis=0, concat_axis=0, tiled=True
    )
    (expert_out,) = call(
        expert_kernel,
        "experts",
        [VMEM] + [HBM] * 6,
        [(HBM, shape((slots, width), bf16))],
        [pltpu.VMEM((width, 2 * units), bf16)] * 2
        + [
            pltpu.VMEM((2 * units, width), bf16),
            pltpu.VMEM((slots, 2 * units), bf16),
            pltpu.VMEM((slots, width), bf16),
            dma((4 * (units // 256) + 2 + COLUMNS,)),
        ],
        32,
    )(arrived.reshape(slots, width), *weights, *others)

    returned = lax.all_to_all(
        expert_out.reshape(ranks, capacity, width), "sp", split_axis=0, concat_axis=0, tiled=True
    )
    (layer_out,) = call(
        functools.partial(combine_kernel, capacity=capacity),
        "combine",
        [VMEM] * 4,
        [(VMEM, shape((half, width), bf16))],
    )(routing, route_weight, returned.reshape(slots, width), updated)
    return layer_out


def solution(mesh):
    placed = (
        P("sp", "tp"),
        P("sp", "tp"),
        P("sp", "tp"),
        P("sp", "tp"),
        P("tp"),
        P("tp"),
        P(("sp", "tp"), None),
        P(),
        P(),
        P(("sp", "tp"), None),
        P(("sp", "tp"), None),
        P("sp", None, "tp"),
        P("sp", None, "tp"),
        P("sp", "tp", None),
    )
    return jax.shard_map(
        body, mesh=mesh, in_specs=placed, out_specs=P(("sp", "tp"), None), check_vma=False
    )
```

```python
import functools

import jax
import jax.numpy as jnp
from jax import lax
from jax.experimental import pallas as pl
from jax.experimental.pallas import tpu as pltpu
from jax.sharding import PartitionSpec as P


HEAD_DIM = 128
TAIL = 8
GROUPS = 4
COLUMNS = 4
epsilon = 1e-06
f32 = jnp.float32
bf16 = jnp.bfloat16

NN = (((1,), (0,)), ((), ()))
NT = (((1,), (1,)), ((), ()))
TN = (((0,), (0,)), ((), ()))


def dot(a, b, dims=NN):
    return lax.dot_general(a, b, dims, preferred_element_type=f32)


def split(x):
    hi = x.astype(bf16)
    return hi, (x - hi.astype(f32)).astype(bf16)


def sigmoid(x):
    return 1.0 / (1.0 + jnp.exp(-x))


def fetch(copies):
    for copy in copies:
        copy.start()
    return copies


def local_kernel(
    q_hbm, f_hbm, v_hbm, low_hbm, w_hbm, intra_ref, qe_ref, out_ref, w_ref, q_ref, f_ref, v_ref, low_ref, sem, *, rows
):
    length, channels = q_ref.shape
    per = HEAD_DIM // rows
    block = channels // GROUPS
    low = pltpu.make_async_copy(low_hbm, low_ref, sem.at[3 * GROUPS])
    low.start()
    copies = []
    for g in range(GROUPS):
        lanes = slice(g * block, (g + 1) * block)
        copies.append(
            fetch(
                [
                    pltpu.make_async_copy(hbm.at[:, lanes], ref.at[:, lanes], sem.at[3 * g + i])
                    for i, (hbm, ref) in enumerate(((f_hbm, f_ref), (q_hbm, q_ref), (v_hbm, v_ref)))
                ]
            )
        )
    ahead = pltpu.make_async_copy(w_hbm, w_ref, sem.at[3 * GROUPS + 1])
    ahead.start()
    t = lax.broadcasted_iota(jnp.int32, (length, length), 0)
    s = lax.broadcasted_iota(jnp.int32, (length, length), 1)
    causal = t >= s
    tri = jnp.where(causal, 1.0, 0.0).astype(bf16)
    place = lax.broadcasted_iota(jnp.int32, (TAIL, HEAD_DIM), 0)
    low.wait()
    for g in range(GROUPS):
        group = slice(g * block, (g + 1) * block)
        for copy in copies[g]:
            copy.wait()
        gap = 1.0 - low_ref[:, group]
        key_gate = gap * sigmoid(-f_ref[:, group].astype(f32))
        hi, lo = split(jnp.log1p(-key_gate))
        total = dot(tri, hi) + dot(tri, lo)
        middle = total[length // 2 - 1 : length // 2]
        last = total[length - 1 : length]
        query = q_ref[:, group].astype(f32)
        scaled_query = (query * jnp.exp(total - middle)).astype(bf16)
        scaled_key = (key_gate * jnp.exp(middle - total)).astype(bf16)
        weighted = (key_gate * jnp.exp(last - total)).astype(bf16)
        qe_ref[:, group] = (query * jnp.exp(total)).astype(bf16)
        last_hi, last_lo = split(last)
        for i in range(block // HEAD_DIM):
            h = g * (block // HEAD_DIM) + i
            inner = slice(i * HEAD_DIM, (i + 1) * HEAD_DIM)
            lanes = slice(h * HEAD_DIM, (h + 1) * HEAD_DIM)
            value = v_ref[:, lanes]
            state = dot(value, weighted[:, inner], TN).astype(bf16)
            scores = dot(scaled_query[:, inner], scaled_key[:, inner], NT)
            scores = jnp.where(causal, scores, 0.0).astype(bf16)
            intra_ref[:, lanes] = dot(scores, value)
            tail = jnp.where(
                place == 0,
                last_hi[:, inner].astype(f32),
                jnp.where(place == 1, last_lo[:, inner].astype(f32), 0.0),
            ).astype(bf16)
            for j in range(per):
                out_ref[h * per + j, :rows] = state[j * rows : (j + 1) * rows]
                out_ref[h * per + j, rows:] = tail
    ahead.wait()


def scan_kernel(in_ref, out_ref, *, rows):
    state = jnp.zeros((rows, HEAD_DIM), f32)
    for i in range(in_ref.shape[0]):
        out_ref[i] = state.astype(bf16)
        tail = in_ref[i, rows:].astype(f32)
        decay = jnp.exp(tail[0:1] + tail[1:2])
        state = state * decay + in_ref[i, :rows].astype(f32)


def mixed_head(h, at, intra_ref, qe_ref, state_ref, gate_ref, gain_ref):
    lanes = slice(h * HEAD_DIM, (h + 1) * HEAD_DIM)
    out = intra_ref[at, lanes] + dot(qe_ref[at, lanes], state_ref[h], NT)
    scale = lax.rsqrt(jnp.mean(out * out, axis=-1, keepdims=True) + epsilon)
    gate = gate_ref[:, lanes].astype(f32)
    return (out * scale * gain_ref[:, lanes] * (gate * sigmoid(gate))).astype(bf16)


def send_kernel(tp_ref, intra_ref, qe_ref, state_ref, gate_hbm, gain_hbm, send_ref, gate_ref, gain_ref, sem):
    half = send_ref.shape[0]
    at = pl.ds(pl.multiple_of((1 - tp_ref[0]) * half, half), half)
    copies = fetch(
        [
            pltpu.make_async_copy(gate_hbm.at[at], gate_ref, sem.at[0]),
            pltpu.make_async_copy(gain_hbm, gain_ref, sem.at[1]),
        ]
    )
    for copy in copies:
        copy.wait()
    for h in range(state_ref.shape[0]):
        lanes = slice(h * HEAD_DIM, (h + 1) * HEAD_DIM)
        send_ref[:, lanes] = mixed_head(h, at, intra_ref, qe_ref, state_ref, gate_ref, gain_ref)


def keep_kernel(
    tp_ref, intra_ref, qe_ref, state_ref, gate_hbm, gain_hbm, w_ref, g_hbm, u_hbm, acc_ref, g_ref, u_ref,
    gate_ref, gain_ref, mix_ref, sem,
):
    channels = mix_ref.shape[1]
    half = mix_ref.shape[0]
    own = tp_ref[0]
    at = pl.ds(pl.multiple_of(own * half, half), half)
    copies = fetch(
        [
            pltpu.make_async_copy(gate_hbm.at[at], gate_ref, sem.at[0]),
            pltpu.make_async_copy(gain_hbm, gain_ref, sem.at[1]),
        ]
    )
    ahead = fetch(
        [
            pltpu.make_async_copy(g_hbm, g_ref, sem.at[2]),
            pltpu.make_async_copy(u_hbm, u_ref, sem.at[3]),
        ]
    )
    for copy in copies:
        copy.wait()
    for h in range(state_ref.shape[0]):
        lanes = slice(h * HEAD_DIM, (h + 1) * HEAD_DIM)
        mix_ref[:, lanes] = mixed_head(h, at, intra_ref, qe_ref, state_ref, gate_ref, gain_ref)
    acc_ref[...] = dot(mix_ref[...], w_ref[pl.ds(pl.multiple_of(own * channels, channels), channels)])
    for copy in ahead:
        copy.wait()


def slots_of(routing, capacity):
    top, count = routing.shape
    s = lax.broadcasted_iota(jnp.int32, (count, count), 0)
    t = lax.broadcasted_iota(jnp.int32, (count, count), 1)
    before = jnp.where(s < t, 1.0, 0.0).astype(bf16)
    place = lax.broadcasted_iota(jnp.int32, (128, count), 0)
    taken = jnp.zeros((128, 1), f32)
    slots = []
    for k in range(top):
        expert = routing[k : k + 1]
        named = jnp.where(place == expert, 1.0, 0.0)
        rank = dot(named.astype(bf16), before) + taken
        rank = jnp.sum(named * rank, axis=0, keepdims=True)
        slots.append(expert * capacity + rank.astype(jnp.int32))
        taken = taken + jnp.sum(named, axis=1, keepdims=True)
    return slots


def project_kernel(
    tp_ref, recv_ref, acc_ref, route_ref, weight_ref, w_ref, res_hbm, gain_hbm, d0_hbm, u1_hbm, d1_hbm,
    upd_ref, hi_ref, lo_ref, box_hbm, d0_ref, u1_ref, d1_ref,
    res_ref, gain_ref, box_ref, sem, *, capacity,
):
    half, width = acc_ref.shape
    channels = recv_ref.shape[1]
    other = 1 - tp_ref[0]
    block = width // COLUMNS
    copies = fetch(
        [
            pltpu.make_async_copy(res_hbm, res_ref, sem.at[0]),
            pltpu.make_async_copy(gain_hbm, gain_ref, sem.at[1]),
        ]
    )
    ahead = fetch(
        [
            pltpu.make_async_copy(hbm, ref, sem.at[2 + COLUMNS + i])
            for i, (hbm, ref) in enumerate(((d0_hbm, d0_ref), (u1_hbm, u1_ref), (d1_hbm, d1_ref)))
        ]
    )
    place = lax.broadcasted_iota(jnp.int32, (box_ref.shape[0], half), 0)
    chosen = jnp.zeros(place.shape, f32)
    weighted = jnp.zeros(place.shape, f32)
    for k, slot in enumerate(slots_of(route_ref[...], capacity)):
        chosen = chosen + jnp.where(place == slot, 1.0, 0.0)
        weighted = weighted + jnp.where(place == slot, weight_ref[k : k + 1], 0.0)
    chosen = chosen.astype(bf16)
    hi_ref[...], lo_ref[...] = split(weighted)
    partial = dot(recv_ref[...], w_ref[pl.ds(pl.multiple_of(other * channels, channels), channels)])
    for copy in copies:
        copy.wait()
    updated = (res_ref[...].astype(f32) + (acc_ref[...] + partial)).astype(bf16)
    upd_ref[...] = updated
    updated = updated.astype(f32)
    scale = lax.rsqrt(jnp.mean(updated * updated, axis=-1, keepdims=True) + epsilon)
    stores = []
    for n in range(COLUMNS):
        lanes = slice(n * block, (n + 1) * block)
        normed = (upd_ref[:, lanes].astype(f32) * scale * gain_ref[:, lanes]).astype(bf16)
        box_ref[:, lanes] = dot(chosen, normed).astype(bf16)
        stores.append(
            pltpu.make_async_copy(box_ref.at[:, lanes], box_hbm.at[:, lanes], sem.at[2 + n])
        )
        stores[n].start()
    for copy in stores:
        copy.wait()
    for copy in ahead:
        copy.wait()


def expert_kernel(x_ref, g0_ref, u0_ref, d0_ref, g1_ref, u1_ref, d1_ref, out_hbm, hid_ref, out_ref, sem):
    units = g0_ref.shape[1]
    width = d0_ref.shape[1]
    block = 256
    x = x_ref[...]
    for side, (g_ref, u_ref) in enumerate(((g0_ref, u0_ref), (g1_ref, u1_ref))):
        for j in range(units // block):
            lanes = slice(j * block, (j + 1) * block)
            gate = dot(x, g_ref[:, lanes])
            hidden = (gate * sigmoid(gate) * dot(x, u_ref[:, lanes])).astype(bf16)
            hid_ref[:, side * units + j * block : side * units + (j + 1) * block] = hidden
    block = width // COLUMNS
    stores = []
    for n in range(COLUMNS):
        lanes = slice(n * block, (n + 1) * block)
        out = dot(hid_ref[:, :units], d0_ref[:, lanes]) + dot(hid_ref[:, units:], d1_ref[:, lanes])
        out_ref[:, lanes] = out.astype(bf16)
        stores.append(pltpu.make_async_copy(out_ref.at[:, lanes], out_hbm.at[:, lanes], sem.at[n]))
        stores[n].start()
    for copy in stores:
        copy.wait()


def combine_kernel(hi_ref, lo_ref, back_ref, upd_ref, out_ref):
    back = back_ref[...]
    out_ref[...] = (
        upd_ref[...].astype(f32) + (dot(hi_ref[...], back, TN) + dot(lo_ref[...], back, TN))
    ).astype(bf16)


HBM = pl.BlockSpec(memory_space=pltpu.HBM)
SMEM = pl.BlockSpec(memory_space=pltpu.SMEM)
VMEM = pl.BlockSpec(memory_space=pltpu.VMEM)
KEPT = pl.BlockSpec(memory_space=pltpu.VMEM)
FIXED = ((HBM, pltpu.HBM), (KEPT, pltpu.VMEM))


def call(kernel, ins, outs, scratch=(), mib=16):
    def fixed(spec):
        return next((space for known, space in FIXED if known is spec), None)

    run = pl.pallas_call(
        kernel,
        in_specs=ins,
        out_specs=[spec for spec, _ in outs],
        out_shape=[
            fixed(spec)(shape.shape, shape.dtype) if fixed(spec) else shape for spec, shape in outs
        ],
        scratch_shapes=list(scratch),
        compiler_params=pltpu.CompilerParams(vmem_limit_bytes=mib * 1024 * 1024),
    )

    def placed(*args):
        return run(
            *(
                pltpu.with_memory_space_constraint(arg, fixed(spec)) if fixed(spec) else arg
                for spec, arg in zip(ins, args)
            )
        )

    return placed


def body(
    query,
    forget_logit,
    value,
    out_gate,
    lower_bound,
    head_gain,
    residual_in,
    w_out,
    ffn_gain,
    routing,
    route_weight,
    expert_gate,
    expert_up,
    expert_down,
):
    shape = jax.ShapeDtypeStruct
    dma = pltpu.SemaphoreType.DMA
    ranks = lax.axis_size("sp")
    sides = lax.axis_size("tp")
    length, channels = query.shape
    heads = channels // HEAD_DIM
    rows = channels // ranks
    half = length // sides
    width = w_out.shape[1]
    top = routing.shape[1]
    capacity = 2 * half * top // ranks
    slots = ranks * capacity
    units = expert_gate.shape[2]
    tp = lax.axis_index("tp").reshape(1)
    swap = [(i, i ^ 1) for i in range(sides)]

    weights = (expert_gate[0], expert_up[0], expert_down[0])
    others = tuple(lax.ppermute(w, "tp", swap) for w in weights)

    intra, qe, packed, w_kept = call(
        functools.partial(local_kernel, rows=rows),
        [HBM] * 5,
        [
            (VMEM, shape((length, channels), f32)),
            (VMEM, shape((length, channels), bf16)),
            (VMEM, shape((ranks, rows + TAIL, HEAD_DIM), bf16)),
            (KEPT, shape(w_out.shape, bf16)),
        ],
        [pltpu.VMEM((length, channels), bf16)] * 3
        + [pltpu.VMEM((1, channels), f32), dma((3 * GROUPS + 2,))],
    )(query, forget_logit, value, lower_bound.reshape(1, -1), w_out)

    packed, tp = lax.optimization_barrier((packed, tp))
    gathered = lax.all_to_all(packed, "sp", split_axis=0, concat_axis=0, tiled=True)
    gathered, others = lax.optimization_barrier((gathered, others))
    (prior,) = call(
        functools.partial(scan_kernel, rows=rows),
        [VMEM],
        [(VMEM, shape((ranks, rows, HEAD_DIM), bf16))],
    )(gathered)
    carried = lax.all_to_all(prior, "sp", split_axis=0, concat_axis=0, tiled=True)

    mix_args = (
        tp,
        intra,
        qe,
        carried.reshape(heads, HEAD_DIM, HEAD_DIM),
        out_gate,
        head_gain.reshape(1, -1),
    )
    mix_specs = [SMEM, VMEM, VMEM, VMEM, HBM, HBM]
    mix_scratch = [pltpu.VMEM((half, channels), bf16), pltpu.VMEM((1, channels), f32)]
    (send,) = call(
        send_kernel, mix_specs, [(VMEM, shape((half, channels), bf16))], mix_scratch + [dma((2,))]
    )(*mix_args)
    recv = lax.ppermute(send, "tp", swap)
    partial, gate_kept, up_kept = call(
        keep_kernel,
        mix_specs + [KEPT, HBM, HBM],
        [(VMEM, shape((half, width), f32))] + [(KEPT, shape((width, units), bf16))] * 2,
        mix_scratch + [pltpu.VMEM((half, channels), bf16), dma((4,))],
    )(*mix_args, w_kept, *weights[:2])
    updated, hi, lo, outbox, *downs = call(
        functools.partial(project_kernel, capacity=capacity),
        [SMEM, VMEM, VMEM, VMEM, VMEM, KEPT] + [HBM] * 5,
        [
            (VMEM, shape((half, width), bf16)),
            (VMEM, shape((slots, half), bf16)),
            (VMEM, shape((slots, half), bf16)),
            (HBM, shape((slots, width), bf16)),
            (KEPT, shape((units, width), bf16)),
            (KEPT, shape((width, units), bf16)),
            (KEPT, shape((units, width), bf16)),
        ],
        [
            pltpu.VMEM((half, width), bf16),
            pltpu.VMEM((1, width), f32),
            pltpu.VMEM((slots, width), bf16),
            dma((5 + COLUMNS,)),
        ],
    )(
        tp,
        recv,
        partial,
        routing.T,
        route_weight.T,
        w_kept,
        residual_in,
        ffn_gain.reshape(1, -1),
        weights[2],
        *others[1:],
    )
    down_kept, other_up, other_down = downs

    arrived = lax.all_to_all(
        outbox.reshape(ranks, capacity, width), "sp", split_axis=0, concat_axis=0, tiled=True
    )
    (expert_out,) = call(
        expert_kernel,
        [VMEM] + [KEPT] * 6,
        [(HBM, shape((slots, width), bf16))],
        [
            pltpu.VMEM((slots, 2 * units), bf16),
            pltpu.VMEM((slots, width), bf16),
            dma((COLUMNS,)),
        ],
    )(arrived.reshape(slots, width), gate_kept, up_kept, down_kept, others[0], other_up, other_down)

    returned = lax.all_to_all(
        expert_out.reshape(ranks, capacity, width), "sp", split_axis=0, concat_axis=0, tiled=True
    )
    (layer_out,) = call(
        combine_kernel, [VMEM] * 4, [(VMEM, shape((half, width), bf16))]
    )(hi, lo, returned.reshape(slots, width), updated)
    return layer_out


def solution(mesh):
    placed = (
        P("sp", "tp"),
        P("sp", "tp"),
        P("sp", "tp"),
        P("sp", "tp"),
        P("tp"),
        P("tp"),
        P(("sp", "tp"), None),
        P(),
        P(),
        P(("sp", "tp"), None),
        P(("sp", "tp"), None),
        P("sp", None, "tp"),
        P("sp", None, "tp"),
        P("sp", "tp", None),
    )

    return jax.shard_map(
        body, mesh=mesh, in_specs=placed, out_specs=P(("sp", "tp"), None), check_vma=False
    )
```

```python
import functools

import jax
import jax.numpy as jnp
from jax import lax
from jax.experimental import pallas as pl
from jax.experimental.pallas import tpu as pltpu
from jax.sharding import PartitionSpec as P


HEAD_DIM = 128
TAIL = 8
GROUP = 4
COLUMNS = 4
epsilon = 1e-06
f32 = jnp.float32
bf16 = jnp.bfloat16

NN = (((1,), (0,)), ((), ()))
NT = (((1,), (1,)), ((), ()))
TN = (((0,), (0,)), ((), ()))


def dot(a, b, dims=NN):
    return lax.dot_general(a, b, dims, preferred_element_type=f32)


def split(x):
    hi = x.astype(bf16)
    return hi, (x - hi.astype(f32)).astype(bf16)


def sigmoid(x):
    return 1.0 / (1.0 + jnp.exp(-x))


def fetch(copies):
    for copy in copies:
        copy.start()
    return copies


def side_of(place_ref):
    return place_ref[0] & 1


def member_of(place_ref):
    return (place_ref[0] >> 1) & (GROUP - 1)


def group_of(place_ref):
    return (place_ref[0] >> 1) // GROUP


def decay_tail(log_decay):
    hi, lo = split(log_decay)
    place = lax.broadcasted_iota(jnp.int32, (TAIL, HEAD_DIM), 0)
    rows = jnp.where(place == 0, hi.astype(f32), jnp.where(place == 1, lo.astype(f32), 0.0))
    return rows.astype(bf16)


def log_decay_of(ref, at, h, heads):
    start = heads * HEAD_DIM + h * TAIL
    rows = ref[at, start : start + TAIL].astype(f32)
    return rows[0:1] + rows[1:2]


def first_kernel(place_ref, f_hbm, v_hbm, low_hbm, *refs):
    outs, (total_ref, key_ref, f_ref, v_ref, low_ref, sem) = refs[:GROUP], refs[GROUP:]
    length, block = f_ref.shape[1:]
    heads = block // HEAD_DIM
    member = member_of(place_ref)
    copies = []
    for k in range(GROUP):
        lanes = pl.ds(pl.multiple_of((member ^ k) * block, block), block)
        copies.append(
            fetch(
                [
                    pltpu.make_async_copy(hbm.at[:, lanes], ref.at[k], sem.at[3 * k + i])
                    for i, (hbm, ref) in enumerate(((f_hbm, f_ref), (low_hbm, low_ref), (v_hbm, v_ref)))
                ]
            )
        )
    t = lax.broadcasted_iota(jnp.int32, (length, length), 0)
    s = lax.broadcasted_iota(jnp.int32, (length, length), 1)
    tri = jnp.where(t >= s, 1.0, 0.0).astype(bf16)
    for k in range(GROUP):
        for copy in copies[k]:
            copy.wait()
        key_gate = (1.0 - low_ref[k]) * sigmoid(-f_ref[k].astype(f32))
        hi, lo = split(jnp.log1p(-key_gate))
        total = dot(tri, hi) + dot(tri, lo)
        last = total[length - 1 : length]
        weighted = (key_gate * jnp.exp(last - total)).astype(bf16)
        total_ref[k] = total
        key_ref[k] = key_gate
        for h in range(heads):
            lanes = slice(h * HEAD_DIM, (h + 1) * HEAD_DIM)
            outs[k][lanes] = dot(v_ref[k, :, lanes], weighted[:, lanes], TN).astype(bf16)
            start = heads * HEAD_DIM + h * TAIL
            outs[k][start : start + TAIL] = decay_tail(last[:, lanes])


def intra_kernel(
    place_ref, total_ref, key_ref, q_hbm, v_hbm, gate_hbm, gain_hbm, w_hbm, intra_ref, qe_ref, gated_ref, w_ref,
    q_ref, v_ref, gate_ref, gain_ref, sem,
):
    length, block = q_ref.shape[1:]
    member = member_of(place_ref)
    copies = []
    for k in range(GROUP):
        lanes = pl.ds(pl.multiple_of((member ^ k) * block, block), block)
        pairs = ((q_hbm, q_ref), (v_hbm, v_ref), (gate_hbm, gate_ref), (gain_hbm, gain_ref))
        copies.append(
            fetch(
                [
                    pltpu.make_async_copy(hbm.at[:, lanes], ref.at[k], sem.at[4 * k + i])
                    for i, (hbm, ref) in enumerate(pairs)
                ]
            )
        )
    ahead = pltpu.make_async_copy(w_hbm, w_ref, sem.at[4 * GROUP])
    ahead.start()
    t = lax.broadcasted_iota(jnp.int32, (length, length), 0)
    s = lax.broadcasted_iota(jnp.int32, (length, length), 1)
    for k in range(GROUP):
        for copy in copies[k]:
            copy.wait()
        total = total_ref[k]
        middle = total[length // 2 - 1 : length // 2]
        query = q_ref[k].astype(f32)
        scaled_query = (query * jnp.exp(total - middle)).astype(bf16)
        scaled_key = (key_ref[k] * jnp.exp(middle - total)).astype(bf16)
        qe_ref[k] = (query * jnp.exp(total)).astype(bf16)
        gate = gate_ref[k].astype(f32)
        gated_ref[k] = gain_ref[k] * (gate * sigmoid(gate))
        for h in range(block // HEAD_DIM):
            lanes = slice(h * HEAD_DIM, (h + 1) * HEAD_DIM)
            scores = dot(scaled_query[:, lanes], scaled_key[:, lanes], NT)
            scores = jnp.where(t >= s, scores, 0.0).astype(bf16)
            intra_ref[k, :, lanes] = dot(scores, v_ref[k, :, lanes])
    ahead.wait()


def total_kernel(place_ref, *refs):
    parts, (out_ref, part_ref) = refs[:GROUP], refs[GROUP:]
    heads = out_ref.shape[0] // (HEAD_DIM + TAIL)
    member = member_of(place_ref)
    for k in range(GROUP):
        part_ref[member ^ k] = parts[k][...]
    for h in range(heads):
        rows = slice(h * HEAD_DIM, (h + 1) * HEAD_DIM)
        state = part_ref[0, rows].astype(f32)
        log_decay = log_decay_of(part_ref, 0, h, heads)
        for j in range(1, GROUP):
            more = log_decay_of(part_ref, j, h, heads)
            state = state * jnp.exp(more) + part_ref[j, rows].astype(f32)
            log_decay = log_decay + more
        out_ref[rows] = state.astype(bf16)
        start = heads * HEAD_DIM + h * TAIL
        out_ref[start : start + TAIL] = decay_tail(log_decay)


def carry_kernel(place_ref, *refs, groups):
    parts, totals = refs[:GROUP], refs[GROUP : GROUP + groups]
    outs, (part_ref, total_ref, state_ref) = refs[GROUP + groups : 2 * GROUP + groups], refs[-3:]
    heads = outs[0].shape[0] // HEAD_DIM
    member = member_of(place_ref)
    group = group_of(place_ref)
    for k in range(GROUP):
        part_ref[member ^ k] = parts[k][...]
    for k in range(groups):
        total_ref[group ^ k] = totals[k][...]
    for h in range(heads):
        rows = slice(h * HEAD_DIM, (h + 1) * HEAD_DIM)

        def one(g, state):
            return state * jnp.exp(log_decay_of(total_ref, g, h, heads)) + total_ref[g, rows].astype(f32)

        state = lax.fori_loop(0, group, one, jnp.zeros((HEAD_DIM, HEAD_DIM), f32))
        for j in range(GROUP):
            state_ref[j, rows] = state.astype(bf16)
            if j + 1 < GROUP:
                state = state * jnp.exp(log_decay_of(part_ref, j, h, heads)) + part_ref[j, rows].astype(f32)
    for k in range(GROUP):
        outs[k][...] = state_ref[member ^ k]


def mixed_rows(out_ref, side, member, intra_ref, qe_ref, gated_ref, states):
    half = out_ref.shape[0]
    block = intra_ref.shape[2]
    at = pl.ds(pl.multiple_of(side * half, half), half)
    for k in range(GROUP):
        mixed = []
        for h in range(block // HEAD_DIM):
            lanes = slice(h * HEAD_DIM, (h + 1) * HEAD_DIM)
            out = intra_ref[k, at, lanes] + dot(qe_ref[k, at, lanes], states[k][lanes], NT)
            scale = lax.rsqrt(jnp.mean(out * out, axis=-1, keepdims=True) + epsilon)
            mixed.append((out * scale * gated_ref[k, at, lanes]).astype(bf16))
        where = pl.ds(pl.multiple_of((member ^ k) * block, block), block)
        out_ref[:, where] = jnp.concatenate(mixed, axis=1)


def send_kernel(place_ref, intra_ref, qe_ref, gated_ref, *refs):
    mixed_rows(refs[GROUP], 1 - side_of(place_ref), member_of(place_ref), intra_ref, qe_ref, gated_ref, refs[:GROUP])


def keep_kernel(place_ref, intra_ref, qe_ref, gated_ref, *refs):
    states, (w_ref, g_hbm, u_hbm, acc_ref, g_ref, u_ref, mix_ref, sem) = refs[:GROUP], refs[GROUP:]
    channels = mix_ref.shape[1]
    own = side_of(place_ref)
    ahead = fetch(
        [
            pltpu.make_async_copy(g_hbm, g_ref, sem.at[0]),
            pltpu.make_async_copy(u_hbm, u_ref, sem.at[1]),
        ]
    )
    mixed_rows(mix_ref, own, member_of(place_ref), intra_ref, qe_ref, gated_ref, states)
    acc_ref[...] = dot(mix_ref[...], w_ref[pl.ds(pl.multiple_of(own * channels, channels), channels)])
    for copy in ahead:
        copy.wait()


def slots_of(routing, capacity):
    top, count = routing.shape
    s = lax.broadcasted_iota(jnp.int32, (count, count), 0)
    t = lax.broadcasted_iota(jnp.int32, (count, count), 1)
    before = jnp.where(s < t, 1.0, 0.0).astype(bf16)
    place = lax.broadcasted_iota(jnp.int32, (128, count), 0)
    taken = jnp.zeros((128, 1), f32)
    slots = []
    for k in range(top):
        expert = routing[k : k + 1]
        named = jnp.where(place == expert, 1.0, 0.0)
        rank = dot(named.astype(bf16), before) + taken
        rank = jnp.sum(named * rank, axis=0, keepdims=True)
        slots.append(expert * capacity + rank.astype(jnp.int32))
        taken = taken + jnp.sum(named, axis=1, keepdims=True)
    return slots


def project_kernel(
    place_ref, recv_ref, acc_ref, route_ref, weight_ref, w_ref, res_hbm, gain_hbm, d0_hbm, u1_hbm, d1_hbm,
    upd_ref, hi_ref, lo_ref, box_ref, d0_ref, u1_ref, d1_ref,
    res_ref, gain_ref, sem, *, capacity,
):
    half, _ = acc_ref.shape
    channels = recv_ref.shape[1]
    other = 1 - side_of(place_ref)
    copies = fetch(
        [
            pltpu.make_async_copy(res_hbm, res_ref, sem.at[0]),
            pltpu.make_async_copy(gain_hbm, gain_ref, sem.at[1]),
        ]
    )
    ahead = fetch(
        [
            pltpu.make_async_copy(hbm, ref, sem.at[2 + i])
            for i, (hbm, ref) in enumerate(((d0_hbm, d0_ref), (u1_hbm, u1_ref), (d1_hbm, d1_ref)))
        ]
    )
    place = lax.broadcasted_iota(jnp.int32, (box_ref.shape[0], half), 0)
    chosen = jnp.zeros(place.shape, f32)
    weighted = jnp.zeros(place.shape, f32)
    for k, slot in enumerate(slots_of(route_ref[...], capacity)):
        chosen = chosen + jnp.where(place == slot, 1.0, 0.0)
        weighted = weighted + jnp.where(place == slot, weight_ref[k : k + 1], 0.0)
    chosen = chosen.astype(bf16)
    hi_ref[...], lo_ref[...] = split(weighted)
    partial = dot(recv_ref[...], w_ref[pl.ds(pl.multiple_of(other * channels, channels), channels)])
    for copy in copies:
        copy.wait()
    updated = (res_ref[...].astype(f32) + (acc_ref[...] + partial)).astype(bf16)
    upd_ref[...] = updated
    updated = updated.astype(f32)
    scale = lax.rsqrt(jnp.mean(updated * updated, axis=-1, keepdims=True) + epsilon)
    normed = (updated * scale * gain_ref[...]).astype(bf16)
    box_ref[...] = dot(chosen, normed).astype(bf16)
    for copy in ahead:
        copy.wait()


def expert_kernel(x_ref, g0_ref, u0_ref, d0_ref, g1_ref, u1_ref, d1_ref, out_ref, hid_ref):
    units = g0_ref.shape[1]
    width = d0_ref.shape[1]
    block = 256
    x = x_ref[...]
    for side, (g_ref, u_ref) in enumerate(((g0_ref, u0_ref), (g1_ref, u1_ref))):
        for j in range(units // block):
            lanes = slice(j * block, (j + 1) * block)
            gate = dot(x, g_ref[:, lanes])
            hidden = (gate * sigmoid(gate) * dot(x, u_ref[:, lanes])).astype(bf16)
            hid_ref[:, side * units + j * block : side * units + (j + 1) * block] = hidden
    block = width // COLUMNS
    for n in range(COLUMNS):
        lanes = slice(n * block, (n + 1) * block)
        out = dot(hid_ref[:, :units], d0_ref[:, lanes]) + dot(hid_ref[:, units:], d1_ref[:, lanes])
        out_ref[:, lanes] = out.astype(bf16)


def combine_kernel(hi_ref, lo_ref, back_ref, upd_ref, out_ref):
    back = back_ref[...]
    out_ref[...] = (
        upd_ref[...].astype(f32) + (dot(hi_ref[...], back, TN) + dot(lo_ref[...], back, TN))
    ).astype(bf16)


HBM = pl.BlockSpec(memory_space=pltpu.HBM)
SMEM = pl.BlockSpec(memory_space=pltpu.SMEM)
VMEM = pl.BlockSpec(memory_space=pltpu.VMEM)
KEPT = pl.BlockSpec(memory_space=pltpu.VMEM)
FIXED = ((HBM, pltpu.HBM), (KEPT, pltpu.VMEM))


def call(kernel, ins, outs, scratch=(), mib=16):
    def fixed(spec):
        return next((space for known, space in FIXED if known is spec), None)

    run = pl.pallas_call(
        kernel,
        in_specs=ins,
        out_specs=[spec for spec, _ in outs],
        out_shape=[
            fixed(spec)(shape.shape, shape.dtype) if fixed(spec) else shape for spec, shape in outs
        ],
        scratch_shapes=list(scratch),
        compiler_params=pltpu.CompilerParams(vmem_limit_bytes=mib * 1024 * 1024),
    )

    def placed(*args):
        return run(
            *(
                pltpu.with_memory_space_constraint(arg, fixed(spec)) if fixed(spec) else arg
                for spec, arg in zip(ins, args)
            )
        )

    return placed


def body(
    query,
    forget_logit,
    value,
    out_gate,
    lower_bound,
    head_gain,
    residual_in,
    w_out,
    ffn_gain,
    routing,
    route_weight,
    expert_gate,
    expert_up,
    expert_down,
):
    shape = jax.ShapeDtypeStruct
    dma = pltpu.SemaphoreType.DMA
    ranks = lax.axis_size("sp")
    sides = lax.axis_size("tp")
    length, channels = query.shape
    part = channels // GROUP
    carried = part + part // HEAD_DIM * TAIL
    groups = ranks // GROUP
    half = length // sides
    width = w_out.shape[1]
    top = routing.shape[1]
    capacity = 2 * half * top // ranks
    slots = ranks * capacity
    units = expert_gate.shape[2]
    rank = lax.axis_index("sp")
    place = (rank * 2 + lax.axis_index("tp")).reshape(1)
    swap = [(i, i ^ 1) for i in range(sides)]

    def away(x, k):
        return lax.ppermute(x, "sp", [(i, i ^ k) for i in range(ranks)])

    weights = (expert_gate[0], expert_up[0], expert_down[0])
    others = tuple(lax.ppermute(w, "tp", swap) for w in weights)

    *states, total, key_gate = call(
        first_kernel,
        [SMEM] + [HBM] * 3,
        [(VMEM, shape((carried, HEAD_DIM), bf16))] * GROUP
        + [(VMEM, shape((GROUP, length, part), f32))] * 2,
        [pltpu.VMEM((GROUP, length, part), bf16)] * 2
        + [pltpu.VMEM((GROUP, 1, part), f32), dma((3 * GROUP,))],
    )(place, forget_logit, value, lower_bound.reshape(1, -1))
    states = states[:1] + [away(states[k], k) for k in range(1, GROUP)]
    intra, qe, gated, w_kept = call(
        intra_kernel,
        [SMEM] + [VMEM] * 2 + [HBM] * 5,
        [
            (VMEM, shape((GROUP, length, part), f32)),
            (VMEM, shape((GROUP, length, part), bf16)),
            (VMEM, shape((GROUP, length, part), f32)),
            (KEPT, shape(w_out.shape, bf16)),
        ],
        [pltpu.VMEM((GROUP, length, part), bf16)] * 3
        + [pltpu.VMEM((GROUP, 1, part), f32), dma((4 * GROUP + 1,))],
    )(place, total, key_gate, query, value, out_gate, head_gain.reshape(1, -1), w_out)
    (totals,) = call(
        total_kernel,
        [SMEM] + [VMEM] * GROUP,
        [(VMEM, shape((carried, HEAD_DIM), bf16))],
        [pltpu.VMEM((GROUP, carried, HEAD_DIM), bf16)],
    )(place, *states)
    totals = [totals] + [away(totals, GROUP * k) for k in range(1, groups)]
    priors = call(
        functools.partial(carry_kernel, groups=groups),
        [SMEM] + [VMEM] * (GROUP + groups),
        [(VMEM, shape((part, HEAD_DIM), bf16))] * GROUP,
        [
            pltpu.VMEM((GROUP, carried, HEAD_DIM), bf16),
            pltpu.VMEM((groups, carried, HEAD_DIM), bf16),
            pltpu.VMEM((GROUP, part, HEAD_DIM), bf16),
        ],
    )(place, *states, *totals)
    priors = list(priors[:1]) + [away(priors[k], k) for k in range(1, GROUP)]

    mix_args = (place, intra, qe, gated, *priors)
    mix_specs = [SMEM] + [VMEM] * (3 + GROUP)
    (send,) = call(send_kernel, mix_specs, [(VMEM, shape((half, channels), bf16))])(*mix_args)
    recv = lax.ppermute(send, "tp", swap)
    partial, gate_kept, up_kept = call(
        keep_kernel,
        mix_specs + [KEPT, HBM, HBM],
        [(VMEM, shape((half, width), f32))] + [(KEPT, shape((width, units), bf16))] * 2,
        [pltpu.VMEM((half, channels), bf16), dma((2,))],
    )(*mix_args, w_kept, *weights[:2])
    recv, others = lax.optimization_barrier((recv, others))
    updated, hi, lo, outbox, down_kept, other_up, other_down = call(
        functools.partial(project_kernel, capacity=capacity),
        [SMEM] + [VMEM] * 4 + [KEPT] + [HBM] * 5,
        [
            (VMEM, shape((half, width), bf16)),
            (VMEM, shape((slots, half), bf16)),
            (VMEM, shape((slots, half), bf16)),
            (VMEM, shape((slots, width), bf16)),
            (KEPT, shape((units, width), bf16)),
            (KEPT, shape((width, units), bf16)),
            (KEPT, shape((units, width), bf16)),
        ],
        [pltpu.VMEM((half, width), bf16), pltpu.VMEM((1, width), f32), dma((5,))],
    )(
        place,
        recv,
        partial,
        routing.T,
        route_weight.T,
        w_kept,
        residual_in,
        ffn_gain.reshape(1, -1),
        weights[2],
        *others[1:],
    )

    arrived = lax.all_to_all(
        outbox.reshape(ranks, capacity, width), "sp", split_axis=0, concat_axis=0, tiled=True
    )
    (expert_out,) = call(
        expert_kernel,
        [VMEM] + [KEPT] * 6,
        [(VMEM, shape((slots, width), bf16))],
        [pltpu.VMEM((slots, 2 * units), bf16)],
    )(arrived.reshape(slots, width), gate_kept, up_kept, down_kept, others[0], other_up, other_down)

    returned = lax.all_to_all(
        expert_out.reshape(ranks, capacity, width), "sp", split_axis=0, concat_axis=0, tiled=True
    )
    (layer_out,) = call(
        combine_kernel, [VMEM] * 4, [(VMEM, shape((half, width), bf16))]
    )(hi, lo, returned.reshape(slots, width), updated)
    return layer_out


def solution(mesh):
    placed = (
        P("sp", "tp"),
        P("sp", "tp"),
        P("sp", "tp"),
        P("sp", "tp"),
        P("tp"),
        P("tp"),
        P(("sp", "tp"), None),
        P(),
        P(),
        P(("sp", "tp"), None),
        P(("sp", "tp"), None),
        P("sp", None, "tp"),
        P("sp", None, "tp"),
        P("sp", "tp", None),
    )

    return jax.shard_map(
        body, mesh=mesh, in_specs=placed, out_specs=P(("sp", "tp"), None), check_vma=False
    )
```

```python
import functools

import jax
import jax.numpy as jnp
from jax import lax
from jax.experimental import pallas as pl
from jax.experimental.pallas import tpu as pltpu
from jax.sharding import PartitionSpec as P


HEAD_DIM = 128
TAIL = 8
GROUP = 4
COLUMNS = 4
epsilon = 1e-06
f32 = jnp.float32
bf16 = jnp.bfloat16

NN = (((1,), (0,)), ((), ()))
NT = (((1,), (1,)), ((), ()))
TN = (((0,), (0,)), ((), ()))


def dot(a, b, dims=NN):
    return lax.dot_general(a, b, dims, preferred_element_type=f32)


def split(x):
    hi = x.astype(bf16)
    return hi, (x - hi.astype(f32)).astype(bf16)


def sigmoid(x):
    return 1.0 / (1.0 + jnp.exp(-x))


def fetch(copies):
    for copy in copies:
        copy.start()
    return copies


def side_of(place_ref):
    return place_ref[0] & 1


def member_of(place_ref):
    return (place_ref[0] >> 1) & (GROUP - 1)


def group_of(place_ref):
    return (place_ref[0] >> 1) // GROUP


def decay_tail(log_decay):
    hi, lo = split(log_decay)
    place = lax.broadcasted_iota(jnp.int32, (TAIL, HEAD_DIM), 0)
    rows = jnp.where(place == 0, hi.astype(f32), jnp.where(place == 1, lo.astype(f32), 0.0))
    return rows.astype(bf16)


def log_decay_of(ref, at, h, heads):
    start = heads * HEAD_DIM + h * TAIL
    rows = ref[at, start : start + TAIL].astype(f32)
    return rows[0:1] + rows[1:2]


def first_kernel(place_ref, f_hbm, v_hbm, low_hbm, *refs):
    outs, (total_ref, key_ref, f_ref, v_ref, low_ref, sem) = refs[:GROUP], refs[GROUP:]
    length, block = f_ref.shape[1:]
    heads = block // HEAD_DIM
    member = member_of(place_ref)
    copies = []
    for k in range(GROUP):
        lanes = pl.ds(pl.multiple_of((member ^ k) * block, block), block)
        copies.append(
            fetch(
                [
                    pltpu.make_async_copy(hbm.at[:, lanes], ref.at[k], sem.at[3 * k + i])
                    for i, (hbm, ref) in enumerate(((f_hbm, f_ref), (low_hbm, low_ref), (v_hbm, v_ref)))
                ]
            )
        )
    t = lax.broadcasted_iota(jnp.int32, (length, length), 0)
    s = lax.broadcasted_iota(jnp.int32, (length, length), 1)
    tri = jnp.where(t >= s, 1.0, 0.0).astype(bf16)
    for k in range(GROUP):
        for copy in copies[k]:
            copy.wait()
        key_gate = (1.0 - low_ref[k]) * sigmoid(-f_ref[k].astype(f32))
        hi, lo = split(jnp.log1p(-key_gate))
        total = dot(tri, hi) + dot(tri, lo)
        last = total[length - 1 : length]
        weighted = (key_gate * jnp.exp(last - total)).astype(bf16)
        total_ref[k] = total
        key_ref[k] = key_gate
        for h in range(heads):
            lanes = slice(h * HEAD_DIM, (h + 1) * HEAD_DIM)
            outs[k][lanes] = dot(v_ref[k, :, lanes], weighted[:, lanes], TN).astype(bf16)
            start = heads * HEAD_DIM + h * TAIL
            outs[k][start : start + TAIL] = decay_tail(last[:, lanes])


def intra_kernel(
    place_ref, total_ref, key_ref, q_hbm, v_hbm, w_hbm, intra_ref, qe_ref, w_ref, q_ref, v_ref, sem
):
    length, block = q_ref.shape[1:]
    member = member_of(place_ref)
    copies = []
    for k in range(GROUP):
        lanes = pl.ds(pl.multiple_of((member ^ k) * block, block), block)
        copies.append(
            fetch(
                [
                    pltpu.make_async_copy(hbm.at[:, lanes], ref.at[k], sem.at[2 * k + i])
                    for i, (hbm, ref) in enumerate(((q_hbm, q_ref), (v_hbm, v_ref)))
                ]
            )
        )
    ahead = side_rows(w_hbm, w_ref, side_of(place_ref), sem.at[2 * GROUP])
    t = lax.broadcasted_iota(jnp.int32, (length, length), 0)
    s = lax.broadcasted_iota(jnp.int32, (length, length), 1)
    for k in range(GROUP):
        for copy in copies[k]:
            copy.wait()
        total = total_ref[k]
        middle = total[length // 2 - 1 : length // 2]
        query = q_ref[k].astype(f32)
        scaled_query = (query * jnp.exp(total - middle)).astype(bf16)
        scaled_key = (key_ref[k] * jnp.exp(middle - total)).astype(bf16)
        qe_ref[k] = (query * jnp.exp(total)).astype(bf16)
        for h in range(block // HEAD_DIM):
            lanes = slice(h * HEAD_DIM, (h + 1) * HEAD_DIM)
            scores = dot(scaled_query[:, lanes], scaled_key[:, lanes], NT)
            scores = jnp.where(t >= s, scores, 0.0).astype(bf16)
            intra_ref[k, :, lanes] = dot(scores, v_ref[k, :, lanes])
    ahead.wait()


def side_rows(hbm, ref, side, sem):
    rows = ref.shape[0]
    copy = pltpu.make_async_copy(hbm.at[pl.ds(pl.multiple_of(side * rows, rows), rows)], ref, sem)
    copy.start()
    return copy


def gate_kernel(place_ref, gate_hbm, gain_hbm, w_hbm, gated_ref, w_ref, gate_ref, gain_ref, sem):
    block = gate_ref.shape[2]
    copies = []
    for k in range(GROUP):
        lanes = pl.ds(pl.multiple_of((member_of(place_ref) ^ k) * block, block), block)
        copies.append(
            fetch(
                [
                    pltpu.make_async_copy(hbm.at[:, lanes], ref.at[k], sem.at[2 * k + i])
                    for i, (hbm, ref) in enumerate(((gate_hbm, gate_ref), (gain_hbm, gain_ref)))
                ]
            )
        )
    ahead = side_rows(w_hbm, w_ref, 1 - side_of(place_ref), sem.at[2 * GROUP])
    for k in range(GROUP):
        for copy in copies[k]:
            copy.wait()
        gate = gate_ref[k].astype(f32)
        gated_ref[k] = gain_ref[k] * (gate * sigmoid(gate))
    ahead.wait()


def bring_kernel(*refs):
    count = len(refs) // 2
    sem = refs[-1]
    copies = fetch(
        [pltpu.make_async_copy(refs[i], refs[count + i], sem.at[i]) for i in range(count)]
    )
    for copy in copies:
        copy.wait()


def total_kernel(place_ref, *refs):
    parts, (out_ref, part_ref) = refs[:GROUP], refs[GROUP:]
    heads = out_ref.shape[0] // (HEAD_DIM + TAIL)
    member = member_of(place_ref)
    for k in range(GROUP):
        part_ref[member ^ k] = parts[k][...]
    for h in range(heads):
        rows = slice(h * HEAD_DIM, (h + 1) * HEAD_DIM)
        state = part_ref[0, rows].astype(f32)
        log_decay = log_decay_of(part_ref, 0, h, heads)
        for j in range(1, GROUP):
            more = log_decay_of(part_ref, j, h, heads)
            state = state * jnp.exp(more) + part_ref[j, rows].astype(f32)
            log_decay = log_decay + more
        out_ref[rows] = state.astype(bf16)
        start = heads * HEAD_DIM + h * TAIL
        out_ref[start : start + TAIL] = decay_tail(log_decay)


def carry_kernel(place_ref, *refs, groups):
    parts, totals = refs[:GROUP], refs[GROUP : GROUP + groups]
    outs, (part_ref, total_ref, state_ref) = refs[GROUP + groups : 2 * GROUP + groups], refs[-3:]
    heads = outs[0].shape[0] // HEAD_DIM
    member = member_of(place_ref)
    group = group_of(place_ref)
    for k in range(GROUP):
        part_ref[member ^ k] = parts[k][...]
    for k in range(groups):
        total_ref[group ^ k] = totals[k][...]
    for h in range(heads):
        rows = slice(h * HEAD_DIM, (h + 1) * HEAD_DIM)

        def one(g, state):
            return state * jnp.exp(log_decay_of(total_ref, g, h, heads)) + total_ref[g, rows].astype(f32)

        state = lax.fori_loop(0, group, one, jnp.zeros((HEAD_DIM, HEAD_DIM), f32))
        for j in range(GROUP):
            state_ref[j, rows] = state.astype(bf16)
            if j + 1 < GROUP:
                state = state * jnp.exp(log_decay_of(part_ref, j, h, heads)) + part_ref[j, rows].astype(f32)
    for k in range(GROUP):
        outs[k][...] = state_ref[member ^ k]


def mixed_rows(out_ref, side, member, intra_ref, qe_ref, gated_ref, states):
    half = out_ref.shape[0]
    block = intra_ref.shape[2]
    at = pl.ds(pl.multiple_of(side * half, half), half)
    for k in range(GROUP):
        mixed = []
        for h in range(block // HEAD_DIM):
            lanes = slice(h * HEAD_DIM, (h + 1) * HEAD_DIM)
            out = intra_ref[k, at, lanes] + dot(qe_ref[k, at, lanes], states[k][lanes], NT)
            scale = lax.rsqrt(jnp.mean(out * out, axis=-1, keepdims=True) + epsilon)
            mixed.append((out * scale * gated_ref[k, at, lanes]).astype(bf16))
        where = pl.ds(pl.multiple_of((member ^ k) * block, block), block)
        out_ref[:, where] = jnp.concatenate(mixed, axis=1)


def send_kernel(place_ref, intra_ref, qe_ref, gated_ref, *refs):
    mixed_rows(refs[GROUP], 1 - side_of(place_ref), member_of(place_ref), intra_ref, qe_ref, gated_ref, refs[:GROUP])


def keep_kernel(place_ref, intra_ref, qe_ref, gated_ref, *refs):
    states, (w_ref, acc_ref, mix_ref) = refs[:GROUP], refs[GROUP:]
    side, member = side_of(place_ref), member_of(place_ref)
    mixed_rows(mix_ref, side, member, intra_ref, qe_ref, gated_ref, states)
    acc_ref[...] = dot(mix_ref[...], w_ref[...])


def slots_of(routing, capacity):
    top, count = routing.shape
    s = lax.broadcasted_iota(jnp.int32, (count, count), 0)
    t = lax.broadcasted_iota(jnp.int32, (count, count), 1)
    before = jnp.where(s < t, 1.0, 0.0).astype(bf16)
    place = lax.broadcasted_iota(jnp.int32, (128, count), 0)
    taken = jnp.zeros((128, 1), f32)
    slots = []
    for k in range(top):
        expert = routing[k : k + 1]
        named = jnp.where(place == expert, 1.0, 0.0)
        rank = dot(named.astype(bf16), before) + taken
        rank = jnp.sum(named * rank, axis=0, keepdims=True)
        slots.append(expert * capacity + rank.astype(jnp.int32))
        taken = taken + jnp.sum(named, axis=1, keepdims=True)
    return slots


def project_kernel(
    place_ref, recv_ref, acc_ref, route_ref, weight_ref, w_ref, res_hbm, gain_hbm, d_hbm,
    upd_ref, hi_ref, lo_ref, d_ref, *refs, capacity,
):
    boxes, (res_ref, gain_ref, sem) = refs[:-3], refs[-3:]
    copies = fetch(
        [
            pltpu.make_async_copy(res_hbm, res_ref, sem.at[0]),
            pltpu.make_async_copy(gain_hbm, gain_ref, sem.at[1]),
        ]
    )
    ahead = pltpu.make_async_copy(d_hbm, d_ref, sem.at[2])
    ahead.start()
    place = lax.broadcasted_iota(jnp.int32, hi_ref.shape, 0)
    chosen = jnp.zeros(place.shape, f32)
    weighted = jnp.zeros(place.shape, f32)
    for k, slot in enumerate(slots_of(route_ref[...] ^ (place_ref[0] >> 1), capacity)):
        chosen = chosen + jnp.where(place == slot, 1.0, 0.0)
        weighted = weighted + jnp.where(place == slot, weight_ref[k : k + 1], 0.0)
    chosen = chosen.astype(bf16)
    hi_ref[...], lo_ref[...] = split(weighted)
    partial = dot(recv_ref[...], w_ref[...])
    for copy in copies:
        copy.wait()
    updated = (res_ref[...].astype(f32) + (acc_ref[...] + partial)).astype(bf16)
    upd_ref[...] = updated
    updated = updated.astype(f32)
    scale = lax.rsqrt(jnp.mean(updated * updated, axis=-1, keepdims=True) + epsilon)
    normed = (updated * scale * gain_ref[...]).astype(bf16)
    box = dot(chosen, normed).astype(bf16)
    rows = box.shape[0] // len(boxes)
    for i, ref in enumerate(boxes):
        ref[...] = box[i * rows : (i + 1) * rows]
    ahead.wait()


def expert_kernel(*refs):
    blocks = (len(refs) - 8) // 2
    weights, (x_ref, hid_ref) = refs[blocks : blocks + 6], refs[-2:]
    g0_ref, u0_ref, d0_ref, g1_ref, u1_ref, d1_ref = weights
    rows = refs[0].shape[0]
    for i in range(blocks):
        x_ref[i * rows : (i + 1) * rows] = refs[i][...]
    units = g0_ref.shape[1]
    width = d0_ref.shape[1]
    block = 256
    x = x_ref[...]
    for side, (g_ref, u_ref) in enumerate(((g0_ref, u0_ref), (g1_ref, u1_ref))):
        for j in range(units // block):
            lanes = slice(j * block, (j + 1) * block)
            gate = dot(x, g_ref[:, lanes])
            hidden = (gate * sigmoid(gate) * dot(x, u_ref[:, lanes])).astype(bf16)
            hid_ref[:, side * units + j * block : side * units + (j + 1) * block] = hidden
    block = width // COLUMNS
    for n in range(COLUMNS):
        lanes = slice(n * block, (n + 1) * block)
        out = dot(hid_ref[:, :units], d0_ref[:, lanes]) + dot(hid_ref[:, units:], d1_ref[:, lanes])
        out = out.astype(bf16)
        for i in range(blocks):
            refs[blocks + 6 + i][:, lanes] = out[i * rows : (i + 1) * rows]


def combine_kernel(base_ref, hi_ref, lo_ref, *refs, start):
    blocks, (out_ref, back_ref) = refs[:-2], refs[-2:]
    rows = blocks[0].shape[0]
    for i, ref in enumerate(blocks):
        back_ref[i * rows : (i + 1) * rows] = ref[...]
    here = slice(start, start + back_ref.shape[0])
    back = back_ref[...]
    total = dot(hi_ref[here], back, TN) + dot(lo_ref[here], back, TN)
    out_ref[...] = (base_ref[...].astype(f32) + total).astype(out_ref.dtype)


HBM = pl.BlockSpec(memory_space=pltpu.HBM)
SMEM = pl.BlockSpec(memory_space=pltpu.SMEM)
VMEM = pl.BlockSpec(memory_space=pltpu.VMEM)
KEPT = pl.BlockSpec(memory_space=pltpu.VMEM)
FIXED = ((HBM, pltpu.HBM), (KEPT, pltpu.VMEM))


def call(kernel, ins, outs, scratch=(), mib=16):
    def fixed(spec):
        return next((space for known, space in FIXED if known is spec), None)

    run = pl.pallas_call(
        kernel,
        in_specs=ins,
        out_specs=[spec for spec, _ in outs],
        out_shape=[
            fixed(spec)(shape.shape, shape.dtype) if fixed(spec) else shape for spec, shape in outs
        ],
        scratch_shapes=list(scratch),
        compiler_params=pltpu.CompilerParams(vmem_limit_bytes=mib * 1024 * 1024),
    )

    def placed(*args):
        return run(
            *(
                pltpu.with_memory_space_constraint(arg, fixed(spec)) if fixed(spec) else arg
                for spec, arg in zip(ins, args)
            )
        )

    return placed


def body(
    query,
    forget_logit,
    value,
    out_gate,
    lower_bound,
    head_gain,
    residual_in,
    w_out,
    ffn_gain,
    routing,
    route_weight,
    expert_gate,
    expert_up,
    expert_down,
):
    shape = jax.ShapeDtypeStruct
    dma = pltpu.SemaphoreType.DMA
    ranks = lax.axis_size("sp")
    sides = lax.axis_size("tp")
    length, channels = query.shape
    part = channels // GROUP
    carried = part + part // HEAD_DIM * TAIL
    groups = ranks // GROUP
    half = length // sides
    width = w_out.shape[1]
    top = routing.shape[1]
    capacity = 2 * half * top // ranks
    slots = ranks * capacity
    units = expert_gate.shape[2]
    rank = lax.axis_index("sp")
    place = (rank * 2 + lax.axis_index("tp")).reshape(1)
    swap = [(i, i ^ 1) for i in range(sides)]

    def away(x, k):
        return lax.ppermute(x, "sp", [(i, i ^ k) for i in range(ranks)])

    weights = (expert_gate[0], expert_up[0], expert_down[0])
    *states, total, key_gate = call(
        first_kernel,
        [SMEM] + [HBM] * 3,
        [(VMEM, shape((carried, HEAD_DIM), bf16))] * GROUP
        + [(VMEM, shape((GROUP, length, part), f32))] * 2,
        [pltpu.VMEM((GROUP, length, part), bf16)] * 2
        + [pltpu.VMEM((GROUP, 1, part), f32), dma((3 * GROUP,))],
    )(place, forget_logit, value, lower_bound.reshape(1, -1))
    states = states[:1] + [away(states[k], k) for k in range(1, GROUP)]
    others = tuple(lax.ppermute(w, "tp", swap) for w in weights)
    intra, qe, w_own = call(
        intra_kernel,
        [SMEM] + [VMEM] * 2 + [HBM] * 3,
        [
            (VMEM, shape((GROUP, length, part), f32)),
            (VMEM, shape((GROUP, length, part), bf16)),
            (KEPT, shape((channels, width), bf16)),
        ],
        [pltpu.VMEM((GROUP, length, part), bf16)] * 2 + [dma((2 * GROUP + 1,))],
    )(place, total, key_gate, query, value, w_out)
    (totals,) = call(
        total_kernel,
        [SMEM] + [VMEM] * GROUP,
        [(VMEM, shape((carried, HEAD_DIM), bf16))],
        [pltpu.VMEM((GROUP, carried, HEAD_DIM), bf16)],
    )(place, *states)
    totals = [totals] + [away(totals, GROUP * k) for k in range(1, groups)]
    gated, w_other = call(
        gate_kernel,
        [SMEM] + [HBM] * 3,
        [(VMEM, shape((GROUP, length, part), f32)), (KEPT, shape((channels, width), bf16))],
        [
            pltpu.VMEM((GROUP, length, part), bf16),
            pltpu.VMEM((GROUP, 1, part), f32),
            dma((2 * GROUP + 1,)),
        ],
    )(place, out_gate, head_gain.reshape(1, -1), w_out)
    priors = call(
        functools.partial(carry_kernel, groups=groups),
        [SMEM] + [VMEM] * (GROUP + groups),
        [(VMEM, shape((part, HEAD_DIM), bf16))] * GROUP,
        [
            pltpu.VMEM((GROUP, carried, HEAD_DIM), bf16),
            pltpu.VMEM((groups, carried, HEAD_DIM), bf16),
            pltpu.VMEM((GROUP, part, HEAD_DIM), bf16),
        ],
    )(place, *states, *totals)
    priors = list(priors[:1]) + [away(priors[k], k) for k in range(1, GROUP)]

    gate_kept, up_kept = call(
        bring_kernel, [HBM] * 2, [(KEPT, shape((width, units), bf16))] * 2, [dma((2,))]
    )(*weights[:2])

    mix_args = (place, intra, qe, gated, *priors)
    mix_specs = [SMEM] + [VMEM] * (3 + GROUP)
    (send,) = call(send_kernel, mix_specs, [(VMEM, shape((half, channels), bf16))])(*mix_args)
    recv = lax.ppermute(send, "tp", swap)
    (partial,) = call(
        keep_kernel,
        mix_specs + [KEPT],
        [(VMEM, shape((half, width), f32))],
        [pltpu.VMEM((half, channels), bf16)],
    )(*mix_args, w_own)
    recv, others = lax.optimization_barrier((recv, others))
    direct = capacity % 16 == 0
    blocks = ranks if direct else 1
    block = shape((slots // blocks, width), bf16)
    updated, hi, lo, down_kept, *boxes = call(
        functools.partial(project_kernel, capacity=capacity),
        [SMEM] + [VMEM] * 4 + [KEPT] + [HBM] * 3,
        [
            (VMEM, shape((half, width), bf16)),
            (VMEM, shape((slots, half), bf16)),
            (VMEM, shape((slots, half), bf16)),
            (KEPT, shape((units, width), bf16)),
        ]
        + [(VMEM, block)] * blocks,
        [pltpu.VMEM((half, width), bf16), pltpu.VMEM((1, width), f32), dma((3,))],
    )(
        place,
        recv,
        partial,
        routing.T,
        route_weight.T,
        w_other,
        residual_in,
        ffn_gain.reshape(1, -1),
        weights[2],
    )
    kept = (gate_kept, up_kept, down_kept, *others)

    def experts(arrays):
        rows = sum(x.shape[0] for x in arrays)
        return call(
            expert_kernel,
            [VMEM] * len(arrays) + [KEPT] * 6,
            [(VMEM, shape(x.shape, bf16)) for x in arrays],
            [pltpu.VMEM((rows, width), bf16), pltpu.VMEM((rows, 2 * units), bf16)],
        )(*arrays, *kept)

    def combine(base, arrays, start, kind):
        rows = sum(x.shape[0] for x in arrays)
        (out,) = call(
            functools.partial(combine_kernel, start=start),
            [VMEM] * (3 + len(arrays)),
            [(VMEM, shape((half, width), kind))],
            [pltpu.VMEM((rows, width), bf16)],
        )(base, hi, lo, *arrays)
        return out

    if not direct:

        def exchange(x):
            order = jnp.arange(ranks, dtype=jnp.int32) ^ rank
            x = jnp.take(x.reshape(ranks, capacity, width), order, axis=0)
            x = lax.all_to_all(x, "sp", split_axis=0, concat_axis=0, tiled=True)
            return jnp.take(x, order, axis=0).reshape(slots, width)

        (result,) = experts([exchange(boxes[0])])
        return combine(updated, [exchange(result)], 0, bf16)

    def moved(arrays, ks):
        out = []
        for k, x in zip(ks, arrays):
            out.append(away(x, k) if k else x)
        return out

    middle = ranks // 2
    near, far = range(middle), range(middle, ranks)
    near_in = moved(boxes[:middle], near)
    far_in = moved(boxes[middle:], far)
    near_out = experts(near_in)
    near_back = moved(near_out, near)
    far_out = experts(far_in)
    far_back = moved(far_out, far)
    base = combine(updated, near_back, 0, f32)
    return combine(base, far_back, middle * capacity, bf16)


def solution(mesh):
    placed = (
        P("sp", "tp"),
        P("sp", "tp"),
        P("sp", "tp"),
        P("sp", "tp"),
        P("tp"),
        P("tp"),
        P(("sp", "tp"), None),
        P(),
        P(),
        P(("sp", "tp"), None),
        P(("sp", "tp"), None),
        P("sp", None, "tp"),
        P("sp", None, "tp"),
        P("sp", "tp", None),
    )

    return jax.shard_map(
        body, mesh=mesh, in_specs=placed, out_specs=P(("sp", "tp"), None), check_vma=False
    )
```

```python
import functools

import jax
import jax.numpy as jnp
from jax import lax
from jax.experimental import pallas as pl
from jax.experimental.pallas import tpu as pltpu
from jax.sharding import PartitionSpec as P


HEAD_DIM = 128
TAIL = 8
GROUP = 4
COLUMNS = 4
epsilon = 1e-06
f32 = jnp.float32
bf16 = jnp.bfloat16

NN = (((1,), (0,)), ((), ()))
NT = (((1,), (1,)), ((), ()))
TN = (((0,), (0,)), ((), ()))


def dot(a, b, dims=NN):
    return lax.dot_general(a, b, dims, preferred_element_type=f32)


def split(x):
    hi = x.astype(bf16)
    return hi, (x - hi.astype(f32)).astype(bf16)


def sigmoid(x):
    return 1.0 / (1.0 + jnp.exp(-x))


def fetch(copies):
    for copy in copies:
        copy.start()
    return copies


def side_of(place_ref):
    return place_ref[0] & 1


def member_of(place_ref):
    return (place_ref[0] >> 1) & (GROUP - 1)


def group_of(place_ref):
    return (place_ref[0] >> 1) // GROUP


def decay_tail(log_decay):
    hi, lo = split(log_decay)
    place = lax.broadcasted_iota(jnp.int32, (TAIL, HEAD_DIM), 0)
    rows = jnp.where(place == 0, hi.astype(f32), jnp.where(place == 1, lo.astype(f32), 0.0))
    return rows.astype(bf16)


def log_decay_of(ref, at, h, heads):
    start = heads * HEAD_DIM + h * TAIL
    rows = ref[at, start : start + TAIL].astype(f32)
    return rows[0:1] + rows[1:2]


def first_kernel(place_ref, f_hbm, v_hbm, low_hbm, *refs):
    outs, (total_ref, key_ref, f_ref, v_ref, low_ref, sem) = refs[:GROUP], refs[GROUP:]
    length, block = f_ref.shape[1:]
    heads = block // HEAD_DIM
    member = member_of(place_ref)
    copies = []
    for k in range(GROUP):
        lanes = pl.ds(pl.multiple_of((member ^ k) * block, block), block)
        copies.append(
            fetch(
                [
                    pltpu.make_async_copy(hbm.at[:, lanes], ref.at[k], sem.at[3 * k + i])
                    for i, (hbm, ref) in enumerate(((f_hbm, f_ref), (low_hbm, low_ref), (v_hbm, v_ref)))
                ]
            )
        )
    t = lax.broadcasted_iota(jnp.int32, (length, length), 0)
    s = lax.broadcasted_iota(jnp.int32, (length, length), 1)
    tri = jnp.where(t >= s, 1.0, 0.0).astype(bf16)
    for k in range(GROUP):
        for copy in copies[k]:
            copy.wait()
        key_gate = (1.0 - low_ref[k]) * sigmoid(-f_ref[k].astype(f32))
        hi, lo = split(jnp.log1p(-key_gate))
        total = dot(tri, hi) + dot(tri, lo)
        last = total[length - 1 : length]
        weighted = (key_gate * jnp.exp(last - total)).astype(bf16)
        total_ref[k] = total
        key_ref[k] = key_gate
        for h in range(heads):
            lanes = slice(h * HEAD_DIM, (h + 1) * HEAD_DIM)
            outs[k][lanes] = dot(v_ref[k, :, lanes], weighted[:, lanes], TN).astype(bf16)
            start = heads * HEAD_DIM + h * TAIL
            outs[k][start : start + TAIL] = decay_tail(last[:, lanes])


def intra_kernel(
    place_ref, total_ref, key_ref, q_hbm, v_hbm, w_hbm, intra_ref, qe_ref, w_ref, q_ref, v_ref, sem
):
    length, block = q_ref.shape[1:]
    member = member_of(place_ref)
    copies = []
    for k in range(GROUP):
        lanes = pl.ds(pl.multiple_of((member ^ k) * block, block), block)
        copies.append(
            fetch(
                [
                    pltpu.make_async_copy(hbm.at[:, lanes], ref.at[k], sem.at[2 * k + i])
                    for i, (hbm, ref) in enumerate(((q_hbm, q_ref), (v_hbm, v_ref)))
                ]
            )
        )
    ahead = side_rows(w_hbm, w_ref, side_of(place_ref), sem.at[2 * GROUP])
    t = lax.broadcasted_iota(jnp.int32, (length, length), 0)
    s = lax.broadcasted_iota(jnp.int32, (length, length), 1)
    for k in range(GROUP):
        for copy in copies[k]:
            copy.wait()
        total = total_ref[k]
        middle = total[length // 2 - 1 : length // 2]
        query = q_ref[k].astype(f32)
        scaled_query = (query * jnp.exp(total - middle)).astype(bf16)
        scaled_key = (key_ref[k] * jnp.exp(middle - total)).astype(bf16)
        qe_ref[k] = (query * jnp.exp(total)).astype(bf16)
        for h in range(block // HEAD_DIM):
            lanes = slice(h * HEAD_DIM, (h + 1) * HEAD_DIM)
            scores = dot(scaled_query[:, lanes], scaled_key[:, lanes], NT)
            scores = jnp.where(t >= s, scores, 0.0).astype(bf16)
            intra_ref[k, :, lanes] = dot(scores, v_ref[k, :, lanes])
    ahead.wait()


def side_rows(hbm, ref, side, sem):
    rows = ref.shape[0]
    copy = pltpu.make_async_copy(hbm.at[pl.ds(pl.multiple_of(side * rows, rows), rows)], ref, sem)
    copy.start()
    return copy


def gate_kernel(place_ref, gate_hbm, gain_hbm, w_hbm, gated_ref, w_ref, gate_ref, gain_ref, sem):
    block = gate_ref.shape[2]
    copies = []
    for k in range(GROUP):
        lanes = pl.ds(pl.multiple_of((member_of(place_ref) ^ k) * block, block), block)
        copies.append(
            fetch(
                [
                    pltpu.make_async_copy(hbm.at[:, lanes], ref.at[k], sem.at[2 * k + i])
                    for i, (hbm, ref) in enumerate(((gate_hbm, gate_ref), (gain_hbm, gain_ref)))
                ]
            )
        )
    ahead = side_rows(w_hbm, w_ref, 1 - side_of(place_ref), sem.at[2 * GROUP])
    for k in range(GROUP):
        for copy in copies[k]:
            copy.wait()
        gate = gate_ref[k].astype(f32)
        gated_ref[k] = gain_ref[k] * (gate * sigmoid(gate))
    ahead.wait()


def bring_kernel(*refs):
    count = len(refs) // 2
    sem = refs[-1]
    copies = fetch(
        [pltpu.make_async_copy(refs[i], refs[count + i], sem.at[i]) for i in range(count)]
    )
    for copy in copies:
        copy.wait()


def total_kernel(place_ref, *refs):
    parts, (out_ref, part_ref) = refs[:GROUP], refs[GROUP:]
    heads = out_ref.shape[0] // (HEAD_DIM + TAIL)
    member = member_of(place_ref)
    for k in range(GROUP):
        part_ref[member ^ k] = parts[k][...]
    for h in range(heads):
        rows = slice(h * HEAD_DIM, (h + 1) * HEAD_DIM)
        state = part_ref[0, rows].astype(f32)
        log_decay = log_decay_of(part_ref, 0, h, heads)
        for j in range(1, GROUP):
            more = log_decay_of(part_ref, j, h, heads)
            state = state * jnp.exp(more) + part_ref[j, rows].astype(f32)
            log_decay = log_decay + more
        out_ref[rows] = state.astype(bf16)
        start = heads * HEAD_DIM + h * TAIL
        out_ref[start : start + TAIL] = decay_tail(log_decay)


def carry_kernel(place_ref, *refs, groups):
    parts, totals = refs[:GROUP], refs[GROUP : GROUP + groups]
    outs, (part_ref, total_ref, state_ref) = refs[GROUP + groups : 2 * GROUP + groups], refs[-3:]
    heads = outs[0].shape[0] // HEAD_DIM
    member = member_of(place_ref)
    group = group_of(place_ref)
    for k in range(GROUP):
        part_ref[member ^ k] = parts[k][...]
    for k in range(groups):
        total_ref[group ^ k] = totals[k][...]
    for h in range(heads):
        rows = slice(h * HEAD_DIM, (h + 1) * HEAD_DIM)

        def one(g, state):
            return state * jnp.exp(log_decay_of(total_ref, g, h, heads)) + total_ref[g, rows].astype(f32)

        state = lax.fori_loop(0, group, one, jnp.zeros((HEAD_DIM, HEAD_DIM), f32))
        for j in range(GROUP):
            state_ref[j, rows] = state.astype(bf16)
            if j + 1 < GROUP:
                state = state * jnp.exp(log_decay_of(part_ref, j, h, heads)) + part_ref[j, rows].astype(f32)
    for k in range(GROUP):
        outs[k][...] = state_ref[member ^ k]


def mixed_rows(out_ref, side, member, intra_ref, qe_ref, gated_ref, states):
    half = out_ref.shape[0]
    block = intra_ref.shape[2]
    at = pl.ds(pl.multiple_of(side * half, half), half)
    for k in range(GROUP):
        mixed = []
        for h in range(block // HEAD_DIM):
            lanes = slice(h * HEAD_DIM, (h + 1) * HEAD_DIM)
            out = intra_ref[k, at, lanes] + dot(qe_ref[k, at, lanes], states[k][lanes], NT)
            scale = lax.rsqrt(jnp.mean(out * out, axis=-1, keepdims=True) + epsilon)
            mixed.append((out * scale * gated_ref[k, at, lanes]).astype(bf16))
        where = pl.ds(pl.multiple_of((member ^ k) * block, block), block)
        out_ref[:, where] = jnp.concatenate(mixed, axis=1)


def send_kernel(place_ref, intra_ref, qe_ref, gated_ref, *refs):
    mixed_rows(refs[GROUP], 1 - side_of(place_ref), member_of(place_ref), intra_ref, qe_ref, gated_ref, refs[:GROUP])


def keep_kernel(place_ref, intra_ref, qe_ref, gated_ref, *refs):
    states, (w_ref, acc_ref, mix_ref) = refs[:GROUP], refs[GROUP:]
    side, member = side_of(place_ref), member_of(place_ref)
    mixed_rows(mix_ref, side, member, intra_ref, qe_ref, gated_ref, states)
    acc_ref[...] = dot(mix_ref[...], w_ref[...])


def slots_of(routing, capacity):
    top, count = routing.shape
    s = lax.broadcasted_iota(jnp.int32, (count, count), 0)
    t = lax.broadcasted_iota(jnp.int32, (count, count), 1)
    before = jnp.where(s < t, 1.0, 0.0).astype(bf16)
    place = lax.broadcasted_iota(jnp.int32, (128, count), 0)
    taken = jnp.zeros((128, 1), f32)
    slots = []
    for k in range(top):
        expert = routing[k : k + 1]
        named = jnp.where(place == expert, 1.0, 0.0)
        rank = dot(named.astype(bf16), before) + taken
        rank = jnp.sum(named * rank, axis=0, keepdims=True)
        slots.append(expert * capacity + rank.astype(jnp.int32))
        taken = taken + jnp.sum(named, axis=1, keepdims=True)
    return slots


def project_kernel(
    recv_ref, acc_ref, w_ref, res_hbm, gain_hbm, d_hbm, upd_ref, norm_ref, d_ref, res_ref, gain_ref, sem
):
    copies = fetch(
        [
            pltpu.make_async_copy(res_hbm, res_ref, sem.at[0]),
            pltpu.make_async_copy(gain_hbm, gain_ref, sem.at[1]),
        ]
    )
    ahead = pltpu.make_async_copy(d_hbm, d_ref, sem.at[2])
    ahead.start()
    partial = dot(recv_ref[...], w_ref[...])
    for copy in copies:
        copy.wait()
    updated = (res_ref[...].astype(f32) + (acc_ref[...] + partial)).astype(bf16)
    upd_ref[...] = updated
    updated = updated.astype(f32)
    scale = lax.rsqrt(jnp.mean(updated * updated, axis=-1, keepdims=True) + epsilon)
    norm_ref[...] = (updated * scale * gain_ref[...]).astype(bf16)
    ahead.wait()


def placed_rows(slots, weights, target, valid):
    chosen = jnp.zeros(target.shape, f32)
    weighted = jnp.zeros(target.shape, f32)
    for k, slot in enumerate(slots):
        match = (target == slot) & valid
        chosen = chosen + jnp.where(match, 1.0, 0.0)
        weighted = weighted + jnp.where(match, weights[k : k + 1], 0.0)
    return chosen.astype(bf16), *split(weighted)


def own_kernel(place_ref, route_ref, weight_ref, norm_ref, box_ref, hi_ref, lo_ref, *, capacity):
    slots = slots_of(route_ref[...] ^ (place_ref[0] >> 1), capacity)
    row = lax.broadcasted_iota(jnp.int32, hi_ref.shape, 0)
    chosen, hi_ref[...], lo_ref[...] = placed_rows(slots, weight_ref[...], row, row >= 0)
    box_ref[...] = dot(chosen, norm_ref[...]).astype(bf16)


def pair_kernel(
    place_ref, route_ref, weight_ref, other_route_ref, other_weight_ref, norm_ref,
    box_ref, chosen_ref, hi_ref, lo_ref, other_hi_ref, other_lo_ref, *, capacity,
):
    rank, side = place_ref[0] >> 1, side_of(place_ref)
    row = lax.broadcasted_iota(jnp.int32, hi_ref.shape, 0)
    core = (row // capacity) % 2
    target = (row // (2 * capacity) * 2 + side) * capacity + row % capacity
    slots = slots_of(route_ref[...] ^ rank, capacity)
    chosen, hi_ref[...], lo_ref[...] = placed_rows(slots, weight_ref[...], target, core == side)
    box_ref[...] = dot(chosen, norm_ref[...]).astype(bf16)
    slots = slots_of(other_route_ref[...] ^ rank, capacity)
    chosen_ref[...], other_hi_ref[...], other_lo_ref[...] = placed_rows(
        slots, other_weight_ref[...], target, core != side
    )


def pack_kernel(box_ref, chosen_ref, norm_ref, *outs):
    box = (box_ref[...].astype(f32) + dot(chosen_ref[...], norm_ref[...])).astype(bf16)
    rows = box.shape[0] // len(outs)
    for i, ref in enumerate(outs):
        ref[...] = box[i * rows : (i + 1) * rows]


def expert_kernel(*refs):
    blocks = (len(refs) - 8) // 2
    weights, (x_ref, hid_ref) = refs[blocks : blocks + 6], refs[-2:]
    g0_ref, u0_ref, d0_ref, g1_ref, u1_ref, d1_ref = weights
    rows = refs[0].shape[0]
    for i in range(blocks):
        x_ref[i * rows : (i + 1) * rows] = refs[i][...]
    units = g0_ref.shape[1]
    width = d0_ref.shape[1]
    block = 256
    x = x_ref[...]
    for side, (g_ref, u_ref) in enumerate(((g0_ref, u0_ref), (g1_ref, u1_ref))):
        for j in range(units // block):
            lanes = slice(j * block, (j + 1) * block)
            gate = dot(x, g_ref[:, lanes])
            hidden = (gate * sigmoid(gate) * dot(x, u_ref[:, lanes])).astype(bf16)
            hid_ref[:, side * units + j * block : side * units + (j + 1) * block] = hidden
    block = width // COLUMNS
    for n in range(COLUMNS):
        lanes = slice(n * block, (n + 1) * block)
        out = dot(hid_ref[:, :units], d0_ref[:, lanes]) + dot(hid_ref[:, units:], d1_ref[:, lanes])
        out = out.astype(bf16)
        for i in range(blocks):
            refs[blocks + 6 + i][:, lanes] = out[i * rows : (i + 1) * rows]


def combine_kernel(*refs, start, count):
    outs, back_ref = refs[-1 - count : -1], refs[-1]
    blocks = refs[3 * count : -1 - count]
    rows = blocks[0].shape[0]
    for i, ref in enumerate(blocks):
        back_ref[i * rows : (i + 1) * rows] = ref[...]
    here = slice(start, start + back_ref.shape[0])
    back = back_ref[...]
    for i, out_ref in enumerate(outs):
        base_ref, hi_ref, lo_ref = refs[3 * i : 3 * i + 3]
        total = dot(hi_ref[here], back, TN) + dot(lo_ref[here], back, TN)
        out_ref[...] = (base_ref[...].astype(f32) + total).astype(out_ref.dtype)


def add_kernel(a_ref, b_ref, out_ref):
    out_ref[...] = (a_ref[...] + b_ref[...].astype(f32)).astype(out_ref.dtype)


HBM = pl.BlockSpec(memory_space=pltpu.HBM)
SMEM = pl.BlockSpec(memory_space=pltpu.SMEM)
VMEM = pl.BlockSpec(memory_space=pltpu.VMEM)
KEPT = pl.BlockSpec(memory_space=pltpu.VMEM)
FIXED = ((HBM, pltpu.HBM), (KEPT, pltpu.VMEM))


def call(kernel, ins, outs, scratch=(), mib=16):
    def fixed(spec):
        return next((space for known, space in FIXED if known is spec), None)

    run = pl.pallas_call(
        kernel,
        in_specs=ins,
        out_specs=[spec for spec, _ in outs],
        out_shape=[
            fixed(spec)(shape.shape, shape.dtype) if fixed(spec) else shape for spec, shape in outs
        ],
        scratch_shapes=list(scratch),
        compiler_params=pltpu.CompilerParams(vmem_limit_bytes=mib * 1024 * 1024),
    )

    def placed(*args):
        return run(
            *(
                pltpu.with_memory_space_constraint(arg, fixed(spec)) if fixed(spec) else arg
                for spec, arg in zip(ins, args)
            )
        )

    return placed


def body(
    query,
    forget_logit,
    value,
    out_gate,
    lower_bound,
    head_gain,
    residual_in,
    w_out,
    ffn_gain,
    routing,
    route_weight,
    expert_gate,
    expert_up,
    expert_down,
):
    shape = jax.ShapeDtypeStruct
    dma = pltpu.SemaphoreType.DMA
    ranks = lax.axis_size("sp")
    sides = lax.axis_size("tp")
    length, channels = query.shape
    part = channels // GROUP
    carried = part + part // HEAD_DIM * TAIL
    groups = ranks // GROUP
    half = length // sides
    width = w_out.shape[1]
    top = routing.shape[1]
    capacity = 2 * half * top // ranks
    slots = ranks * capacity
    units = expert_gate.shape[2]
    rank = lax.axis_index("sp")
    place = (rank * 2 + lax.axis_index("tp")).reshape(1)
    swap = [(i, i ^ 1) for i in range(sides)]

    def away(x, k):
        return lax.ppermute(x, "sp", [(i, i ^ k) for i in range(ranks)])

    weights = (expert_gate[0], expert_up[0], expert_down[0])
    *states, total, key_gate = call(
        first_kernel,
        [SMEM] + [HBM] * 3,
        [(VMEM, shape((carried, HEAD_DIM), bf16))] * GROUP
        + [(VMEM, shape((GROUP, length, part), f32))] * 2,
        [pltpu.VMEM((GROUP, length, part), bf16)] * 2
        + [pltpu.VMEM((GROUP, 1, part), f32), dma((3 * GROUP,))],
    )(place, forget_logit, value, lower_bound.reshape(1, -1))
    states = states[:1] + [away(states[k], k) for k in range(1, GROUP)]
    others = tuple(lax.ppermute(w, "tp", swap) for w in weights)
    route, weight = routing.T, route_weight.T
    other_route = lax.ppermute(route, "tp", swap)
    other_weight = lax.ppermute(weight, "tp", swap)
    intra, qe, w_own = call(
        intra_kernel,
        [SMEM] + [VMEM] * 2 + [HBM] * 3,
        [
            (VMEM, shape((GROUP, length, part), f32)),
            (VMEM, shape((GROUP, length, part), bf16)),
            (KEPT, shape((channels, width), bf16)),
        ],
        [pltpu.VMEM((GROUP, length, part), bf16)] * 2 + [dma((2 * GROUP + 1,))],
    )(place, total, key_gate, query, value, w_out)
    (totals,) = call(
        total_kernel,
        [SMEM] + [VMEM] * GROUP,
        [(VMEM, shape((carried, HEAD_DIM), bf16))],
        [pltpu.VMEM((GROUP, carried, HEAD_DIM), bf16)],
    )(place, *states)
    totals = [totals] + [away(totals, GROUP * k) for k in range(1, groups)]
    gated, w_other = call(
        gate_kernel,
        [SMEM] + [HBM] * 3,
        [(VMEM, shape((GROUP, length, part), f32)), (KEPT, shape((channels, width), bf16))],
        [
            pltpu.VMEM((GROUP, length, part), bf16),
            pltpu.VMEM((GROUP, 1, part), f32),
            dma((2 * GROUP + 1,)),
        ],
    )(place, out_gate, head_gain.reshape(1, -1), w_out)
    priors = call(
        functools.partial(carry_kernel, groups=groups),
        [SMEM] + [VMEM] * (GROUP + groups),
        [(VMEM, shape((part, HEAD_DIM), bf16))] * GROUP,
        [
            pltpu.VMEM((GROUP, carried, HEAD_DIM), bf16),
            pltpu.VMEM((groups, carried, HEAD_DIM), bf16),
            pltpu.VMEM((GROUP, part, HEAD_DIM), bf16),
        ],
    )(place, *states, *totals)
    priors = list(priors[:1]) + [away(priors[k], k) for k in range(1, GROUP)]

    gate_kept, up_kept = call(
        bring_kernel, [HBM] * 2, [(KEPT, shape((width, units), bf16))] * 2, [dma((2,))]
    )(*weights[:2])

    mix_args = (place, intra, qe, gated, *priors)
    mix_specs = [SMEM] + [VMEM] * (3 + GROUP)
    (send,) = call(send_kernel, mix_specs, [(VMEM, shape((half, channels), bf16))])(*mix_args)
    recv = lax.ppermute(send, "tp", swap)
    (partial,) = call(
        keep_kernel,
        mix_specs + [KEPT],
        [(VMEM, shape((half, width), f32))],
        [pltpu.VMEM((half, channels), bf16)],
    )(*mix_args, w_own)
    recv, others, other_route, other_weight = lax.optimization_barrier(
        (recv, others, other_route, other_weight)
    )
    updated, normed, down_kept = call(
        project_kernel,
        [VMEM] * 2 + [KEPT] + [HBM] * 3,
        [(VMEM, shape((half, width), bf16))] * 2 + [(KEPT, shape((units, width), bf16))],
        [pltpu.VMEM((half, width), bf16), pltpu.VMEM((1, width), f32), dma((3,))],
    )(recv, partial, w_other, residual_in, ffn_gain.reshape(1, -1), weights[2])
    kept = (gate_kept, up_kept, down_kept, *others)
    box = (VMEM, shape((slots, width), bf16))
    table = (VMEM, shape((slots, half), bf16))

    def experts(arrays):
        rows = sum(x.shape[0] for x in arrays)
        return call(
            expert_kernel,
            [VMEM] * len(arrays) + [KEPT] * 6,
            [(VMEM, shape(x.shape, bf16)) for x in arrays],
            [pltpu.VMEM((rows, width), bf16), pltpu.VMEM((rows, 2 * units), bf16)],
        )(*arrays, *kept)

    def combine(sums, arrays, start, kind):
        rows = sum(x.shape[0] for x in arrays)
        return call(
            functools.partial(combine_kernel, start=start, count=len(sums)),
            [VMEM] * (3 * len(sums) + len(arrays)),
            [(VMEM, shape((half, width), kind))] * len(sums),
            [pltpu.VMEM((rows, width), bf16)],
        )(*(x for entry in sums for x in entry), *arrays)

    if capacity % 16:

        def exchange(x):
            order = jnp.arange(ranks, dtype=jnp.int32) ^ rank
            x = jnp.take(x.reshape(ranks, capacity, width), order, axis=0)
            x = lax.all_to_all(x, "sp", split_axis=0, concat_axis=0, tiled=True)
            return jnp.take(x, order, axis=0).reshape(slots, width)

        outbox, hi, lo = call(
            functools.partial(own_kernel, capacity=capacity),
            [SMEM] + [VMEM] * 3,
            [box, table, table],
        )(place, route, weight, normed)
        (result,) = experts([exchange(outbox)])
        return combine([(updated, hi, lo)], [exchange(result)], 0, bf16)[0]

    other_normed = lax.ppermute(normed, "tp", swap)
    own_box, chosen, hi, lo, other_hi, other_lo = call(
        functools.partial(pair_kernel, capacity=capacity), [SMEM] + [VMEM] * 5, [box] + [table] * 5
    )(place, route, weight, other_route, other_weight, normed)
    blocks = ranks // 2
    boxes = call(
        pack_kernel, [VMEM] * 3, [(VMEM, shape((2 * capacity, width), bf16))] * blocks
    )(own_box, chosen, other_normed)

    def paired(x, j):
        pairs = [
            (i * sides + side, (i ^ (2 * j + side)) * sides + side)
            for i in range(ranks)
            for side in range(sides)
        ]
        return lax.ppermute(x, ("sp", "tp"), pairs)

    near = list(range(blocks // 2))
    early = list(range(blocks // 2, blocks * 3 // 4))
    late = list(range(blocks * 3 // 4, blocks))
    arrived = [paired(x, j) for j, x in enumerate(boxes)]
    back = [None] * blocks
    for group in (early, near, late):
        for j, x in zip(group, experts([arrived[j] for j in group])):
            back[j] = paired(x, j)
    zero = jnp.zeros((half, width), bf16)
    own, other = combine(
        [(updated, hi, lo), (zero, other_hi, other_lo)], [back[j] for j in near], 0, f32
    )
    start = len(near) * 2 * capacity
    rest = [back[j] for j in early + late]
    (other,) = combine([(other, other_hi, other_lo)], rest, start, bf16)
    extra = lax.ppermute(other, "tp", swap)
    (own,) = combine([(own, hi, lo)], rest, start, f32)
    (layer_out,) = call(add_kernel, [VMEM] * 2, [(VMEM, shape((half, width), bf16))])(own, extra)
    return layer_out


def solution(mesh):
    placed = (
        P("sp", "tp"),
        P("sp", "tp"),
        P("sp", "tp"),
        P("sp", "tp"),
        P("tp"),
        P("tp"),
        P(("sp", "tp"), None),
        P(),
        P(),
        P(("sp", "tp"), None),
        P(("sp", "tp"), None),
        P("sp", None, "tp"),
        P("sp", None, "tp"),
        P("sp", "tp", None),
    )

    return jax.shard_map(
        body, mesh=mesh, in_specs=placed, out_specs=P(("sp", "tp"), None), check_vma=False
    )
```

```python
import functools

import jax
import jax.numpy as jnp
from jax import lax
from jax.experimental import pallas as pl
from jax.experimental.pallas import tpu as pltpu
from jax.sharding import PartitionSpec as P


HEAD_DIM = 128
TAIL = 8
GROUP = 4
COLUMNS = 4
epsilon = 1e-06
f32 = jnp.float32
bf16 = jnp.bfloat16

NN = (((1,), (0,)), ((), ()))
NT = (((1,), (1,)), ((), ()))
TN = (((0,), (0,)), ((), ()))


def dot(a, b, dims=NN):
    return lax.dot_general(a, b, dims, preferred_element_type=f32)


def split(x):
    hi = x.astype(bf16)
    return hi, (x - hi.astype(f32)).astype(bf16)


def sigmoid(x):
    return 1.0 / (1.0 + jnp.exp(-x))


def fetch(copies):
    for copy in copies:
        copy.start()
    return copies


def side_of(place_ref):
    return place_ref[0] & 1


def member_of(place_ref):
    return (place_ref[0] >> 1) & (GROUP - 1)


def group_of(place_ref):
    return (place_ref[0] >> 1) // GROUP


def decay_tail(log_decay):
    hi, lo = split(log_decay)
    place = lax.broadcasted_iota(jnp.int32, (TAIL, HEAD_DIM), 0)
    rows = jnp.where(place == 0, hi.astype(f32), jnp.where(place == 1, lo.astype(f32), 0.0))
    return rows.astype(bf16)


def log_decay_of(ref, at, h, heads):
    start = heads * HEAD_DIM + h * TAIL
    rows = ref[at, start : start + TAIL].astype(f32)
    return rows[0:1] + rows[1:2]


def first_kernel(place_ref, f_hbm, v_hbm, low_hbm, *refs):
    outs, (total_ref, key_ref, f_ref, v_ref, low_ref, sem) = refs[:GROUP], refs[GROUP:]
    length, block = f_ref.shape[1:]
    heads = block // HEAD_DIM
    member = member_of(place_ref)
    copies = []
    for k in range(GROUP):
        lanes = pl.ds(pl.multiple_of((member ^ k) * block, block), block)
        copies.append(
            fetch(
                [
                    pltpu.make_async_copy(hbm.at[:, lanes], ref.at[k], sem.at[3 * k + i])
                    for i, (hbm, ref) in enumerate(((f_hbm, f_ref), (low_hbm, low_ref), (v_hbm, v_ref)))
                ]
            )
        )
    t = lax.broadcasted_iota(jnp.int32, (length, length), 0)
    s = lax.broadcasted_iota(jnp.int32, (length, length), 1)
    tri = jnp.where(t >= s, 1.0, 0.0).astype(bf16)
    for k in range(GROUP):
        copies[k][0].wait()
        copies[k][1].wait()
    weighted, last = [], []
    for k in range(GROUP):
        key_gate = (1.0 - low_ref[k]) * sigmoid(-f_ref[k].astype(f32))
        hi, lo = split(jnp.log1p(-key_gate))
        total = dot(tri, hi) + dot(tri, lo)
        last.append(total[length - 1 : length])
        weighted.append((key_gate * jnp.exp(last[k] - total)).astype(bf16))
        total_ref[k] = total
        key_ref[k] = key_gate
    for k in range(GROUP):
        copies[k][2].wait()
    for k in range(GROUP):
        for h in range(heads):
            lanes = slice(h * HEAD_DIM, (h + 1) * HEAD_DIM)
            outs[k][lanes] = dot(v_ref[k, :, lanes], weighted[k][:, lanes], TN).astype(bf16)
            start = heads * HEAD_DIM + h * TAIL
            outs[k][start : start + TAIL] = decay_tail(last[k][:, lanes])


def intra_kernel(
    place_ref, total_ref, key_ref, q_hbm, v_hbm, w_hbm, intra_ref, qe_ref, own_ref, other_ref, q_ref, v_ref, sem
):
    length, block = q_ref.shape[1:]
    member = member_of(place_ref)
    copies = []
    for k in range(GROUP):
        lanes = pl.ds(pl.multiple_of((member ^ k) * block, block), block)
        copies.append(
            fetch(
                [
                    pltpu.make_async_copy(hbm.at[:, lanes], ref.at[k], sem.at[2 * k + i])
                    for i, (hbm, ref) in enumerate(((q_hbm, q_ref), (v_hbm, v_ref)))
                ]
            )
        )
    side = side_of(place_ref)
    ahead = [
        side_rows(w_hbm, own_ref, side, sem.at[2 * GROUP]),
        side_rows(w_hbm, other_ref, 1 - side, sem.at[2 * GROUP + 1]),
    ]
    t = lax.broadcasted_iota(jnp.int32, (length, length), 0)
    s = lax.broadcasted_iota(jnp.int32, (length, length), 1)
    for k in range(GROUP):
        for copy in copies[k]:
            copy.wait()
        total = total_ref[k]
        middle = total[length // 2 - 1 : length // 2]
        query = q_ref[k].astype(f32)
        scaled_query = (query * jnp.exp(total - middle)).astype(bf16)
        scaled_key = (key_ref[k] * jnp.exp(middle - total)).astype(bf16)
        qe_ref[k] = (query * jnp.exp(total)).astype(bf16)
        for h in range(block // HEAD_DIM):
            lanes = slice(h * HEAD_DIM, (h + 1) * HEAD_DIM)
            scores = dot(scaled_query[:, lanes], scaled_key[:, lanes], NT)
            scores = jnp.where(t >= s, scores, 0.0).astype(bf16)
            intra_ref[k, :, lanes] = dot(scores, v_ref[k, :, lanes])
    for copy in ahead:
        copy.wait()


def side_rows(hbm, ref, side, sem):
    rows = ref.shape[0]
    copy = pltpu.make_async_copy(hbm.at[pl.ds(pl.multiple_of(side * rows, rows), rows)], ref, sem)
    copy.start()
    return copy


def gate_kernel(
    place_ref, gate_hbm, gain_hbm, res_hbm, norm_gain_hbm, d_hbm,
    gated_ref, res_ref, norm_gain_ref, d_ref, gate_ref, gain_ref, sem,
):
    block = gate_ref.shape[2]
    copies = []
    for k in range(GROUP):
        lanes = pl.ds(pl.multiple_of((member_of(place_ref) ^ k) * block, block), block)
        copies.append(
            fetch(
                [
                    pltpu.make_async_copy(hbm.at[:, lanes], ref.at[k], sem.at[2 * k + i])
                    for i, (hbm, ref) in enumerate(((gate_hbm, gate_ref), (gain_hbm, gain_ref)))
                ]
            )
        )
    ahead = fetch(
        [
            pltpu.make_async_copy(hbm, ref, sem.at[2 * GROUP + i])
            for i, (hbm, ref) in enumerate(
                ((res_hbm, res_ref), (norm_gain_hbm, norm_gain_ref), (d_hbm, d_ref))
            )
        ]
    )
    for k in range(GROUP):
        for copy in copies[k]:
            copy.wait()
        gate = gate_ref[k].astype(f32)
        gated_ref[k] = gain_ref[k] * (gate * sigmoid(gate))
    for copy in ahead:
        copy.wait()


def bring_kernel(*refs):
    count = len(refs) // 2
    sem = refs[-1]
    copies = fetch(
        [pltpu.make_async_copy(refs[i], refs[count + i], sem.at[i]) for i in range(count)]
    )
    for copy in copies:
        copy.wait()


def total_kernel(place_ref, *refs):
    parts, (out_ref, part_ref) = refs[:GROUP], refs[GROUP:]
    heads = out_ref.shape[0] // (HEAD_DIM + TAIL)
    member = member_of(place_ref)
    for k in range(GROUP):
        part_ref[member ^ k] = parts[k][...]
    for h in range(heads):
        rows = slice(h * HEAD_DIM, (h + 1) * HEAD_DIM)
        state = part_ref[0, rows].astype(f32)
        log_decay = log_decay_of(part_ref, 0, h, heads)
        for j in range(1, GROUP):
            more = log_decay_of(part_ref, j, h, heads)
            state = state * jnp.exp(more) + part_ref[j, rows].astype(f32)
            log_decay = log_decay + more
        out_ref[rows] = state.astype(bf16)
        start = heads * HEAD_DIM + h * TAIL
        out_ref[start : start + TAIL] = decay_tail(log_decay)


def carry_kernel(place_ref, *refs, groups):
    parts, totals = refs[:GROUP], refs[GROUP : GROUP + groups]
    outs, (part_ref, total_ref, state_ref) = refs[GROUP + groups : 2 * GROUP + groups], refs[-3:]
    heads = outs[0].shape[0] // HEAD_DIM
    member = member_of(place_ref)
    group = group_of(place_ref)
    for k in range(GROUP):
        part_ref[member ^ k] = parts[k][...]
    for k in range(groups):
        total_ref[group ^ k] = totals[k][...]
    for h in range(heads):
        rows = slice(h * HEAD_DIM, (h + 1) * HEAD_DIM)

        def one(g, state):
            return state * jnp.exp(log_decay_of(total_ref, g, h, heads)) + total_ref[g, rows].astype(f32)

        state = lax.fori_loop(0, group, one, jnp.zeros((HEAD_DIM, HEAD_DIM), f32))
        for j in range(GROUP):
            state_ref[j, rows] = state.astype(bf16)
            if j + 1 < GROUP:
                state = state * jnp.exp(log_decay_of(part_ref, j, h, heads)) + part_ref[j, rows].astype(f32)
    for k in range(GROUP):
        outs[k][...] = state_ref[member ^ k]


def mixed_rows(out_ref, side, member, intra_ref, qe_ref, gated_ref, states):
    half = out_ref.shape[0]
    block = intra_ref.shape[2]
    at = pl.ds(pl.multiple_of(side * half, half), half)
    for k in range(GROUP):
        mixed = []
        for h in range(block // HEAD_DIM):
            lanes = slice(h * HEAD_DIM, (h + 1) * HEAD_DIM)
            out = intra_ref[k, at, lanes] + dot(qe_ref[k, at, lanes], states[k][lanes], NT)
            scale = lax.rsqrt(jnp.mean(out * out, axis=-1, keepdims=True) + epsilon)
            mixed.append((out * scale * gated_ref[k, at, lanes]).astype(bf16))
        where = pl.ds(pl.multiple_of((member ^ k) * block, block), block)
        out_ref[:, where] = jnp.concatenate(mixed, axis=1)


def send_kernel(place_ref, intra_ref, qe_ref, gated_ref, *refs):
    mixed_rows(refs[GROUP], 1 - side_of(place_ref), member_of(place_ref), intra_ref, qe_ref, gated_ref, refs[:GROUP])


def keep_kernel(place_ref, intra_ref, qe_ref, gated_ref, *refs):
    states, (w_ref, acc_ref, mix_ref) = refs[:GROUP], refs[GROUP:]
    side, member = side_of(place_ref), member_of(place_ref)
    mixed_rows(mix_ref, side, member, intra_ref, qe_ref, gated_ref, states)
    acc_ref[...] = dot(mix_ref[...], w_ref[...])


def slots_of(routing, capacity):
    top, count = routing.shape
    s = lax.broadcasted_iota(jnp.int32, (count, count), 0)
    t = lax.broadcasted_iota(jnp.int32, (count, count), 1)
    before = jnp.where(s < t, 1.0, 0.0).astype(bf16)
    place = lax.broadcasted_iota(jnp.int32, (128, count), 0)
    taken = jnp.zeros((128, 1), f32)
    slots = []
    for k in range(top):
        expert = routing[k : k + 1]
        named = jnp.where(place == expert, 1.0, 0.0)
        rank = dot(named.astype(bf16), before) + taken
        rank = jnp.sum(named * rank, axis=0, keepdims=True)
        slots.append(expert * capacity + rank.astype(jnp.int32))
        taken = taken + jnp.sum(named, axis=1, keepdims=True)
    return slots


def project_kernel(recv_ref, acc_ref, w_ref, res_ref, gain_ref, upd_ref, norm_ref):
    partial = dot(recv_ref[...], w_ref[...])
    updated = (res_ref[...].astype(f32) + (acc_ref[...] + partial)).astype(bf16)
    upd_ref[...] = updated
    updated = updated.astype(f32)
    scale = lax.rsqrt(jnp.mean(updated * updated, axis=-1, keepdims=True) + epsilon)
    norm_ref[...] = (updated * scale * gain_ref[...]).astype(bf16)


def placed_rows(slots, weights, target, valid):
    chosen = jnp.zeros(target.shape, f32)
    weighted = jnp.zeros(target.shape, f32)
    for k, slot in enumerate(slots):
        match = (target == slot) & valid
        chosen = chosen + jnp.where(match, 1.0, 0.0)
        weighted = weighted + jnp.where(match, weights[k : k + 1], 0.0)
    return chosen.astype(bf16), *split(weighted)


def own_kernel(place_ref, route_ref, weight_ref, norm_ref, box_ref, hi_ref, lo_ref, *, capacity):
    slots = slots_of(route_ref[...] ^ (place_ref[0] >> 1), capacity)
    row = lax.broadcasted_iota(jnp.int32, hi_ref.shape, 0)
    chosen, hi_ref[...], lo_ref[...] = placed_rows(slots, weight_ref[...], row, row >= 0)
    box_ref[...] = dot(chosen, norm_ref[...]).astype(bf16)


def pair_kernel(
    place_ref, route_ref, weight_ref, other_route_ref, other_weight_ref, norm_ref,
    box_ref, chosen_ref, hi_ref, lo_ref, other_hi_ref, other_lo_ref, *, capacity,
):
    rank, side = place_ref[0] >> 1, side_of(place_ref)
    row = lax.broadcasted_iota(jnp.int32, hi_ref.shape, 0)
    core = (row // capacity) % 2
    target = (row // (2 * capacity) * 2 + side) * capacity + row % capacity
    slots = slots_of(route_ref[...] ^ rank, capacity)
    chosen, hi_ref[...], lo_ref[...] = placed_rows(slots, weight_ref[...], target, core == side)
    box_ref[...] = dot(chosen, norm_ref[...]).astype(bf16)
    slots = slots_of(other_route_ref[...] ^ rank, capacity)
    chosen_ref[...], other_hi_ref[...], other_lo_ref[...] = placed_rows(
        slots, other_weight_ref[...], target, core != side
    )


def pack_kernel(box_ref, chosen_ref, norm_ref, *outs):
    box = (box_ref[...].astype(f32) + dot(chosen_ref[...], norm_ref[...])).astype(bf16)
    rows = box.shape[0] // len(outs)
    for i, ref in enumerate(outs):
        ref[...] = box[i * rows : (i + 1) * rows]


def expert_kernel(*refs):
    blocks = (len(refs) - 8) // 2
    weights, (x_ref, hid_ref) = refs[blocks : blocks + 6], refs[-2:]
    g0_ref, u0_ref, d0_ref, g1_ref, u1_ref, d1_ref = weights
    rows = refs[0].shape[0]
    for i in range(blocks):
        x_ref[i * rows : (i + 1) * rows] = refs[i][...]
    units = g0_ref.shape[1]
    width = d0_ref.shape[1]
    block = 256
    x = x_ref[...]
    for side, (g_ref, u_ref) in enumerate(((g0_ref, u0_ref), (g1_ref, u1_ref))):
        for j in range(units // block):
            lanes = slice(j * block, (j + 1) * block)
            gate = dot(x, g_ref[:, lanes])
            hidden = (gate * sigmoid(gate) * dot(x, u_ref[:, lanes])).astype(bf16)
            hid_ref[:, side * units + j * block : side * units + (j + 1) * block] = hidden
    block = width // COLUMNS
    for n in range(COLUMNS):
        lanes = slice(n * block, (n + 1) * block)
        out = dot(hid_ref[:, :units], d0_ref[:, lanes]) + dot(hid_ref[:, units:], d1_ref[:, lanes])
        out = out.astype(bf16)
        for i in range(blocks):
            refs[blocks + 6 + i][:, lanes] = out[i * rows : (i + 1) * rows]


def combine_kernel(*refs, start, count):
    outs, back_ref = refs[-1 - count : -1], refs[-1]
    blocks = refs[3 * count : -1 - count]
    rows = blocks[0].shape[0]
    for i, ref in enumerate(blocks):
        back_ref[i * rows : (i + 1) * rows] = ref[...]
    here = slice(start, start + back_ref.shape[0])
    back = back_ref[...]
    for i, out_ref in enumerate(outs):
        base_ref, hi_ref, lo_ref = refs[3 * i : 3 * i + 3]
        total = dot(hi_ref[here], back, TN) + dot(lo_ref[here], back, TN)
        out_ref[...] = (base_ref[...].astype(f32) + total).astype(out_ref.dtype)


def add_kernel(a_ref, b_ref, out_ref):
    out_ref[...] = (a_ref[...] + b_ref[...].astype(f32)).astype(out_ref.dtype)


HBM = pl.BlockSpec(memory_space=pltpu.HBM)
SMEM = pl.BlockSpec(memory_space=pltpu.SMEM)
VMEM = pl.BlockSpec(memory_space=pltpu.VMEM)
KEPT = pl.BlockSpec(memory_space=pltpu.VMEM)
FIXED = ((HBM, pltpu.HBM), (KEPT, pltpu.VMEM))


def call(kernel, ins, outs, scratch=(), mib=16):
    def fixed(spec):
        return next((space for known, space in FIXED if known is spec), None)

    run = pl.pallas_call(
        kernel,
        in_specs=ins,
        out_specs=[spec for spec, _ in outs],
        out_shape=[
            fixed(spec)(shape.shape, shape.dtype) if fixed(spec) else shape for spec, shape in outs
        ],
        scratch_shapes=list(scratch),
        compiler_params=pltpu.CompilerParams(vmem_limit_bytes=mib * 1024 * 1024),
    )

    def placed(*args):
        return run(
            *(
                pltpu.with_memory_space_constraint(arg, fixed(spec)) if fixed(spec) else arg
                for spec, arg in zip(ins, args)
            )
        )

    return placed


def body(
    query,
    forget_logit,
    value,
    out_gate,
    lower_bound,
    head_gain,
    residual_in,
    w_out,
    ffn_gain,
    routing,
    route_weight,
    expert_gate,
    expert_up,
    expert_down,
):
    shape = jax.ShapeDtypeStruct
    dma = pltpu.SemaphoreType.DMA
    ranks = lax.axis_size("sp")
    sides = lax.axis_size("tp")
    length, channels = query.shape
    part = channels // GROUP
    carried = part + part // HEAD_DIM * TAIL
    groups = ranks // GROUP
    half = length // sides
    width = w_out.shape[1]
    top = routing.shape[1]
    capacity = 2 * half * top // ranks
    slots = ranks * capacity
    units = expert_gate.shape[2]
    rank = lax.axis_index("sp")
    place = (rank * 2 + lax.axis_index("tp")).reshape(1)
    swap = [(i, i ^ 1) for i in range(sides)]

    def away(x, k):
        return lax.ppermute(x, "sp", [(i, i ^ k) for i in range(ranks)])

    weights = (expert_gate[0], expert_up[0], expert_down[0])
    *states, total, key_gate = call(
        first_kernel,
        [SMEM] + [HBM] * 3,
        [(VMEM, shape((carried, HEAD_DIM), bf16))] * GROUP
        + [(VMEM, shape((GROUP, length, part), f32))] * 2,
        [pltpu.VMEM((GROUP, length, part), bf16)] * 2
        + [pltpu.VMEM((GROUP, 1, part), f32), dma((3 * GROUP,))],
    )(place, forget_logit, value, lower_bound.reshape(1, -1))
    states = states[:1] + [away(states[k], k) for k in range(1, GROUP)]
    others = tuple(lax.ppermute(w, "tp", swap) for w in weights)
    route, weight = routing.T, route_weight.T
    other_route = lax.ppermute(route, "tp", swap)
    other_weight = lax.ppermute(weight, "tp", swap)
    gated, residual, norm_gain, down_kept = call(
        gate_kernel,
        [SMEM] + [HBM] * 5,
        [
            (VMEM, shape((GROUP, length, part), f32)),
            (KEPT, shape((half, width), bf16)),
            (KEPT, shape((1, width), f32)),
            (KEPT, shape((units, width), bf16)),
        ],
        [
            pltpu.VMEM((GROUP, length, part), bf16),
            pltpu.VMEM((GROUP, 1, part), f32),
            dma((2 * GROUP + 3,)),
        ],
    )(place, out_gate, head_gain.reshape(1, -1), residual_in, ffn_gain.reshape(1, -1), weights[2])
    (totals,) = call(
        total_kernel,
        [SMEM] + [VMEM] * GROUP,
        [(VMEM, shape((carried, HEAD_DIM), bf16))],
        [pltpu.VMEM((GROUP, carried, HEAD_DIM), bf16)],
    )(place, *states)
    totals = [totals] + [away(totals, GROUP * k) for k in range(1, groups)]
    intra, qe, w_own, w_other = call(
        intra_kernel,
        [SMEM] + [VMEM] * 2 + [HBM] * 3,
        [
            (VMEM, shape((GROUP, length, part), f32)),
            (VMEM, shape((GROUP, length, part), bf16)),
            (KEPT, shape((channels, width), bf16)),
            (KEPT, shape((channels, width), bf16)),
        ],
        [pltpu.VMEM((GROUP, length, part), bf16)] * 2 + [dma((2 * GROUP + 2,))],
    )(place, total, key_gate, query, value, w_out)
    priors = call(
        functools.partial(carry_kernel, groups=groups),
        [SMEM] + [VMEM] * (GROUP + groups),
        [(VMEM, shape((part, HEAD_DIM), bf16))] * GROUP,
        [
            pltpu.VMEM((GROUP, carried, HEAD_DIM), bf16),
            pltpu.VMEM((groups, carried, HEAD_DIM), bf16),
            pltpu.VMEM((GROUP, part, HEAD_DIM), bf16),
        ],
    )(place, *states, *totals)
    priors = list(priors[:1]) + [away(priors[k], k) for k in range(1, GROUP)]

    gate_kept, up_kept = call(
        bring_kernel, [HBM] * 2, [(KEPT, shape((width, units), bf16))] * 2, [dma((2,))]
    )(*weights[:2])

    mix_args = (place, intra, qe, gated, *priors)
    mix_specs = [SMEM] + [VMEM] * (3 + GROUP)
    (send,) = call(send_kernel, mix_specs, [(VMEM, shape((half, channels), bf16))])(*mix_args)
    recv = lax.ppermute(send, "tp", swap)
    (partial,) = call(
        keep_kernel,
        mix_specs + [KEPT],
        [(VMEM, shape((half, width), f32))],
        [pltpu.VMEM((half, channels), bf16)],
    )(*mix_args, w_own)
    recv, others, other_route, other_weight = lax.optimization_barrier(
        (recv, others, other_route, other_weight)
    )
    updated, normed = call(
        project_kernel, [VMEM] * 2 + [KEPT] * 3, [(VMEM, shape((half, width), bf16))] * 2
    )(recv, partial, w_other, residual, norm_gain)
    kept = (gate_kept, up_kept, down_kept, *others)
    box = (VMEM, shape((slots, width), bf16))
    table = (VMEM, shape((slots, half), bf16))

    def experts(arrays):
        rows = sum(x.shape[0] for x in arrays)
        return call(
            expert_kernel,
            [VMEM] * len(arrays) + [KEPT] * 6,
            [(VMEM, shape(x.shape, bf16)) for x in arrays],
            [pltpu.VMEM((rows, width), bf16), pltpu.VMEM((rows, 2 * units), bf16)],
        )(*arrays, *kept)

    def combine(sums, arrays, start, kind):
        rows = sum(x.shape[0] for x in arrays)
        return call(
            functools.partial(combine_kernel, start=start, count=len(sums)),
            [VMEM] * (3 * len(sums) + len(arrays)),
            [(VMEM, shape((half, width), kind))] * len(sums),
            [pltpu.VMEM((rows, width), bf16)],
        )(*(x for entry in sums for x in entry), *arrays)

    if capacity % 16:

        def exchange(x):
            order = jnp.arange(ranks, dtype=jnp.int32) ^ rank
            x = jnp.take(x.reshape(ranks, capacity, width), order, axis=0)
            x = lax.all_to_all(x, "sp", split_axis=0, concat_axis=0, tiled=True)
            return jnp.take(x, order, axis=0).reshape(slots, width)

        outbox, hi, lo = call(
            functools.partial(own_kernel, capacity=capacity),
            [SMEM] + [VMEM] * 3,
            [box, table, table],
        )(place, route, weight, normed)
        (result,) = experts([exchange(outbox)])
        return combine([(updated, hi, lo)], [exchange(result)], 0, bf16)[0]

    other_normed = lax.ppermute(normed, "tp", swap)
    own_box, chosen, hi, lo, other_hi, other_lo = call(
        functools.partial(pair_kernel, capacity=capacity), [SMEM] + [VMEM] * 5, [box] + [table] * 5
    )(place, route, weight, other_route, other_weight, normed)
    blocks = ranks // 2
    boxes = call(
        pack_kernel, [VMEM] * 3, [(VMEM, shape((2 * capacity, width), bf16))] * blocks
    )(own_box, chosen, other_normed)

    def paired(x, j):
        pairs = [
            (i * sides + side, (i ^ (2 * j + side)) * sides + side)
            for i in range(ranks)
            for side in range(sides)
        ]
        return lax.ppermute(x, ("sp", "tp"), pairs)

    near = list(range(blocks // 2))
    early = list(range(blocks // 2, blocks * 3 // 4))
    late = list(range(blocks * 3 // 4, blocks))
    arrived = [paired(x, j) for j, x in enumerate(boxes)]
    back = [None] * blocks
    for group in (early, near, late):
        for j, x in zip(group, experts([arrived[j] for j in group])):
            back[j] = paired(x, j)
    zero = jnp.zeros((half, width), bf16)
    own, other = combine(
        [(updated, hi, lo), (zero, other_hi, other_lo)], [back[j] for j in near], 0, f32
    )
    start = len(near) * 2 * capacity
    rest = [back[j] for j in early + late]
    (other,) = combine([(other, other_hi, other_lo)], rest, start, bf16)
    extra = lax.ppermute(other, "tp", swap)
    (own,) = combine([(own, hi, lo)], rest, start, f32)
    (layer_out,) = call(add_kernel, [VMEM] * 2, [(VMEM, shape((half, width), bf16))])(own, extra)
    return layer_out


def solution(mesh):
    placed = (
        P("sp", "tp"),
        P("sp", "tp"),
        P("sp", "tp"),
        P("sp", "tp"),
        P("tp"),
        P("tp"),
        P(("sp", "tp"), None),
        P(),
        P(),
        P(("sp", "tp"), None),
        P(("sp", "tp"), None),
        P("sp", None, "tp"),
        P("sp", None, "tp"),
        P("sp", "tp", None),
    )

    return jax.shard_map(
        body, mesh=mesh, in_specs=placed, out_specs=P(("sp", "tp"), None), check_vma=False
    )
```

```python
import functools

import jax
import jax.numpy as jnp
from jax import lax
from jax.experimental import pallas as pl
from jax.experimental.pallas import tpu as pltpu
from jax.sharding import PartitionSpec as P


HEAD_DIM = 128
TAIL = 8
GROUP = 4
COLUMNS = 4
epsilon = 1e-06
f32 = jnp.float32
bf16 = jnp.bfloat16

NN = (((1,), (0,)), ((), ()))
NT = (((1,), (1,)), ((), ()))
TN = (((0,), (0,)), ((), ()))


def dot(a, b, dims=NN):
    return lax.dot_general(a, b, dims, preferred_element_type=f32)


def split(x):
    hi = x.astype(bf16)
    return hi, (x - hi.astype(f32)).astype(bf16)


def sigmoid(x):
    return 1.0 / (1.0 + jnp.exp(-x))


def fetch(copies):
    for copy in copies:
        copy.start()
    return copies


def side_of(place_ref):
    return place_ref[0] & 1


def member_of(place_ref):
    return (place_ref[0] >> 1) & (GROUP - 1)


def group_of(place_ref):
    return (place_ref[0] >> 1) // GROUP


def decay_tail(log_decay):
    hi, lo = split(log_decay)
    place = lax.broadcasted_iota(jnp.int32, (TAIL, HEAD_DIM), 0)
    rows = jnp.where(place == 0, hi.astype(f32), jnp.where(place == 1, lo.astype(f32), 0.0))
    return rows.astype(bf16)


def log_decay_of(ref, at, h, heads):
    start = heads * HEAD_DIM + h * TAIL
    rows = ref[at, start : start + TAIL].astype(f32)
    return rows[0:1] + rows[1:2]


def first_kernel(place_ref, f_hbm, v_hbm, low_hbm, *refs):
    outs, (total_ref, key_ref, f_ref, v_ref, low_ref, sem) = refs[:GROUP], refs[GROUP:]
    length, block = f_ref.shape[1:]
    heads = block // HEAD_DIM
    member = member_of(place_ref)
    copies = []
    for k in range(GROUP):
        lanes = pl.ds(pl.multiple_of((member ^ k) * block, block), block)
        copies.append(
            fetch(
                [
                    pltpu.make_async_copy(hbm.at[:, lanes], ref.at[k], sem.at[3 * k + i])
                    for i, (hbm, ref) in enumerate(((f_hbm, f_ref), (low_hbm, low_ref), (v_hbm, v_ref)))
                ]
            )
        )
    t = lax.broadcasted_iota(jnp.int32, (length, length), 0)
    s = lax.broadcasted_iota(jnp.int32, (length, length), 1)
    tri = jnp.where(t >= s, 1.0, 0.0).astype(bf16)
    for k in range(GROUP):
        copies[k][0].wait()
        copies[k][1].wait()
    weighted, last = [], []
    for k in range(GROUP):
        key_gate = (1.0 - low_ref[k]) * sigmoid(-f_ref[k].astype(f32))
        hi, lo = split(jnp.log1p(-key_gate))
        total = dot(tri, hi) + dot(tri, lo)
        last.append(total[length - 1 : length])
        weighted.append((key_gate * jnp.exp(last[k] - total)).astype(bf16))
        total_ref[k] = total
        key_ref[k] = key_gate
    for k in range(GROUP):
        copies[k][2].wait()
    for k in range(GROUP):
        for h in range(heads):
            lanes = slice(h * HEAD_DIM, (h + 1) * HEAD_DIM)
            outs[k][lanes] = dot(v_ref[k, :, lanes], weighted[k][:, lanes], TN).astype(bf16)
            start = heads * HEAD_DIM + h * TAIL
            outs[k][start : start + TAIL] = decay_tail(last[k][:, lanes])


def intra_kernel(
    place_ref, total_ref, key_ref, q_hbm, v_hbm, w_hbm, intra_ref, qe_ref, own_ref, other_ref, q_ref, v_ref, sem
):
    length, block = q_ref.shape[1:]
    member = member_of(place_ref)
    copies = []
    for k in range(GROUP):
        lanes = pl.ds(pl.multiple_of((member ^ k) * block, block), block)
        copies.append(
            fetch(
                [
                    pltpu.make_async_copy(hbm.at[:, lanes], ref.at[k], sem.at[2 * k + i])
                    for i, (hbm, ref) in enumerate(((q_hbm, q_ref), (v_hbm, v_ref)))
                ]
            )
        )
    side = side_of(place_ref)
    ahead = [
        side_rows(w_hbm, own_ref, side, sem.at[2 * GROUP]),
        side_rows(w_hbm, other_ref, 1 - side, sem.at[2 * GROUP + 1]),
    ]
    t = lax.broadcasted_iota(jnp.int32, (length, length), 0)
    s = lax.broadcasted_iota(jnp.int32, (length, length), 1)
    for k in range(GROUP):
        for copy in copies[k]:
            copy.wait()
        total = total_ref[k]
        middle = total[length // 2 - 1 : length // 2]
        query = q_ref[k].astype(f32)
        scaled_query = (query * jnp.exp(total - middle)).astype(bf16)
        scaled_key = (key_ref[k] * jnp.exp(middle - total)).astype(bf16)
        qe_ref[k] = (query * jnp.exp(total)).astype(bf16)
        for h in range(block // HEAD_DIM):
            lanes = slice(h * HEAD_DIM, (h + 1) * HEAD_DIM)
            scores = dot(scaled_query[:, lanes], scaled_key[:, lanes], NT)
            scores = jnp.where(t >= s, scores, 0.0).astype(bf16)
            intra_ref[k, :, lanes] = dot(scores, v_ref[k, :, lanes])
    for copy in ahead:
        copy.wait()


def side_rows(hbm, ref, side, sem):
    rows = ref.shape[0]
    copy = pltpu.make_async_copy(hbm.at[pl.ds(pl.multiple_of(side * rows, rows), rows)], ref, sem)
    copy.start()
    return copy


def gate_kernel(
    place_ref, gate_hbm, gain_hbm, res_hbm, norm_gain_hbm, d_hbm,
    gated_ref, res_ref, norm_gain_ref, d_ref, gate_ref, gain_ref, sem,
):
    block = gate_ref.shape[2]
    copies = []
    for k in range(GROUP):
        lanes = pl.ds(pl.multiple_of((member_of(place_ref) ^ k) * block, block), block)
        copies.append(
            fetch(
                [
                    pltpu.make_async_copy(hbm.at[:, lanes], ref.at[k], sem.at[2 * k + i])
                    for i, (hbm, ref) in enumerate(((gate_hbm, gate_ref), (gain_hbm, gain_ref)))
                ]
            )
        )
    ahead = fetch(
        [
            pltpu.make_async_copy(hbm, ref, sem.at[2 * GROUP + i])
            for i, (hbm, ref) in enumerate(
                ((res_hbm, res_ref), (norm_gain_hbm, norm_gain_ref), (d_hbm, d_ref))
            )
        ]
    )
    for k in range(GROUP):
        for copy in copies[k]:
            copy.wait()
        gate = gate_ref[k].astype(f32)
        gated_ref[k] = gain_ref[k] * (gate * sigmoid(gate))
    for copy in ahead:
        copy.wait()


def bring_kernel(*refs):
    count = len(refs) // 2
    sem = refs[-1]
    copies = fetch(
        [pltpu.make_async_copy(refs[i], refs[count + i], sem.at[i]) for i in range(count)]
    )
    for copy in copies:
        copy.wait()


def total_kernel(place_ref, *refs):
    parts, (out_ref, part_ref) = refs[:GROUP], refs[GROUP:]
    heads = out_ref.shape[0] // (HEAD_DIM + TAIL)
    member = member_of(place_ref)
    for k in range(GROUP):
        part_ref[member ^ k] = parts[k][...]
    for h in range(heads):
        rows = slice(h * HEAD_DIM, (h + 1) * HEAD_DIM)
        state = part_ref[0, rows].astype(f32)
        log_decay = log_decay_of(part_ref, 0, h, heads)
        for j in range(1, GROUP):
            more = log_decay_of(part_ref, j, h, heads)
            state = state * jnp.exp(more) + part_ref[j, rows].astype(f32)
            log_decay = log_decay + more
        out_ref[rows] = state.astype(bf16)
        start = heads * HEAD_DIM + h * TAIL
        out_ref[start : start + TAIL] = decay_tail(log_decay)


def carry_kernel(place_ref, *refs, groups):
    parts, totals = refs[:GROUP], refs[GROUP : GROUP + groups]
    outs, (part_ref, total_ref, state_ref) = refs[GROUP + groups : 2 * GROUP + groups], refs[-3:]
    heads = outs[0].shape[0] // HEAD_DIM
    member = member_of(place_ref)
    group = group_of(place_ref)
    for k in range(GROUP):
        part_ref[member ^ k] = parts[k][...]
    for k in range(groups):
        total_ref[group ^ k] = totals[k][...]
    for h in range(heads):
        rows = slice(h * HEAD_DIM, (h + 1) * HEAD_DIM)

        def one(g, state):
            return state * jnp.exp(log_decay_of(total_ref, g, h, heads)) + total_ref[g, rows].astype(f32)

        state = lax.fori_loop(0, group, one, jnp.zeros((HEAD_DIM, HEAD_DIM), f32))
        for j in range(GROUP):
            state_ref[j, rows] = state.astype(bf16)
            if j + 1 < GROUP:
                state = state * jnp.exp(log_decay_of(part_ref, j, h, heads)) + part_ref[j, rows].astype(f32)
    for k in range(GROUP):
        outs[k][...] = state_ref[member ^ k]


def mix_kernel(place_ref, intra_ref, qe_ref, gated_ref, *refs):
    states, out_ref = refs[:GROUP], refs[GROUP]
    block = intra_ref.shape[2]
    member = member_of(place_ref)
    for k in range(GROUP):
        mixed = []
        for h in range(block // HEAD_DIM):
            lanes = slice(h * HEAD_DIM, (h + 1) * HEAD_DIM)
            out = intra_ref[k, :, lanes] + dot(qe_ref[k, :, lanes], states[k][lanes], NT)
            scale = lax.rsqrt(jnp.mean(out * out, axis=-1, keepdims=True) + epsilon)
            mixed.append((out * scale * gated_ref[k, :, lanes]).astype(bf16))
        where = pl.ds(pl.multiple_of((member ^ k) * block, block), block)
        out_ref[:, where] = jnp.concatenate(mixed, axis=1)


def keep_kernel(mix_ref, w_ref, acc_ref):
    acc_ref[...] = dot(mix_ref[...], w_ref[...])


def slots_of(routing, capacity):
    top, count = routing.shape
    s = lax.broadcasted_iota(jnp.int32, (count, count), 0)
    t = lax.broadcasted_iota(jnp.int32, (count, count), 1)
    before = jnp.where(s < t, 1.0, 0.0).astype(bf16)
    place = lax.broadcasted_iota(jnp.int32, (128, count), 0)
    taken = jnp.zeros((128, 1), f32)
    slots = []
    for k in range(top):
        expert = routing[k : k + 1]
        named = jnp.where(place == expert, 1.0, 0.0)
        rank = dot(named.astype(bf16), before) + taken
        rank = jnp.sum(named * rank, axis=0, keepdims=True)
        slots.append(expert * capacity + rank.astype(jnp.int32))
        taken = taken + jnp.sum(named, axis=1, keepdims=True)
    return slots


def project_kernel(
    place_ref, recv_ref, acc_ref, w_ref, res_ref, other_res_ref, gain_ref, *refs, count
):
    chosen, upd_ref, outs, sum_ref = refs[:count], refs[count], refs[count + 1 : -1], refs[-1]
    half, _ = upd_ref.shape
    side = side_of(place_ref)
    sum_ref[...] = acc_ref[...] + dot(recv_ref[...], w_ref[...])

    def normed_rows(rows_ref, which):
        at = pl.ds(pl.multiple_of(which * half, half), half)
        updated = (rows_ref[...].astype(f32) + sum_ref[at]).astype(bf16)
        wide = updated.astype(f32)
        scale = lax.rsqrt(jnp.mean(wide * wide, axis=-1, keepdims=True) + epsilon)
        return updated, (wide * scale * gain_ref[...]).astype(bf16)

    upd_ref[...], own = normed_rows(res_ref, side)
    if not count:
        outs[0][...] = own
    else:
        _, other = normed_rows(other_res_ref, 1 - side)
        box = (dot(chosen[0][...], own) + dot(chosen[1][...], other)).astype(bf16)
        rows = box.shape[0] // len(outs)
        for i, ref in enumerate(outs):
            ref[...] = box[i * rows : (i + 1) * rows]


def placed_rows(slots, weights, target, valid):
    chosen = jnp.zeros(target.shape, f32)
    weighted = jnp.zeros(target.shape, f32)
    for k, slot in enumerate(slots):
        match = (target == slot) & valid
        chosen = chosen + jnp.where(match, 1.0, 0.0)
        weighted = weighted + jnp.where(match, weights[k : k + 1], 0.0)
    return chosen.astype(bf16), *split(weighted)


def own_kernel(place_ref, route_ref, weight_ref, norm_ref, box_ref, hi_ref, lo_ref, *, capacity):
    slots = slots_of(route_ref[...] ^ (place_ref[0] >> 1), capacity)
    row = lax.broadcasted_iota(jnp.int32, hi_ref.shape, 0)
    chosen, hi_ref[...], lo_ref[...] = placed_rows(slots, weight_ref[...], row, row >= 0)
    box_ref[...] = dot(chosen, norm_ref[...]).astype(bf16)


def pair_kernel(
    place_ref, route_ref, weight_ref, other_route_ref, other_weight_ref,
    chosen_ref, other_chosen_ref, hi_ref, lo_ref, other_hi_ref, other_lo_ref, *, capacity,
):
    rank, side = place_ref[0] >> 1, side_of(place_ref)
    row = lax.broadcasted_iota(jnp.int32, hi_ref.shape, 0)
    core = (row // capacity) % 2
    target = (row // (2 * capacity) * 2 + side) * capacity + row % capacity
    slots = slots_of(route_ref[...] ^ rank, capacity)
    chosen_ref[...], hi_ref[...], lo_ref[...] = placed_rows(slots, weight_ref[...], target, core == side)
    slots = slots_of(other_route_ref[...] ^ rank, capacity)
    other_chosen_ref[...], other_hi_ref[...], other_lo_ref[...] = placed_rows(
        slots, other_weight_ref[...], target, core != side
    )


def expert_kernel(*refs):
    blocks = (len(refs) - 8) // 2
    weights, (x_ref, hid_ref) = refs[blocks : blocks + 6], refs[-2:]
    g0_ref, u0_ref, d0_ref, g1_ref, u1_ref, d1_ref = weights
    rows = refs[0].shape[0]
    for i in range(blocks):
        x_ref[i * rows : (i + 1) * rows] = refs[i][...]
    units = g0_ref.shape[1]
    width = d0_ref.shape[1]
    block = 256
    x = x_ref[...]
    for side, (g_ref, u_ref) in enumerate(((g0_ref, u0_ref), (g1_ref, u1_ref))):
        for j in range(units // block):
            lanes = slice(j * block, (j + 1) * block)
            gate = dot(x, g_ref[:, lanes])
            hidden = (gate * sigmoid(gate) * dot(x, u_ref[:, lanes])).astype(bf16)
            hid_ref[:, side * units + j * block : side * units + (j + 1) * block] = hidden
    block = width // COLUMNS
    for n in range(COLUMNS):
        lanes = slice(n * block, (n + 1) * block)
        out = dot(hid_ref[:, :units], d0_ref[:, lanes]) + dot(hid_ref[:, units:], d1_ref[:, lanes])
        out = out.astype(bf16)
        for i in range(blocks):
            refs[blocks + 6 + i][:, lanes] = out[i * rows : (i + 1) * rows]


def combine_kernel(*refs, start, count):
    outs, back_ref = refs[-1 - count : -1], refs[-1]
    blocks = refs[3 * count : -1 - count]
    rows = blocks[0].shape[0]
    for i, ref in enumerate(blocks):
        back_ref[i * rows : (i + 1) * rows] = ref[...]
    here = slice(start, start + back_ref.shape[0])
    back = back_ref[...]
    for i, out_ref in enumerate(outs):
        base_ref, hi_ref, lo_ref = refs[3 * i : 3 * i + 3]
        total = dot(hi_ref[here], back, TN) + dot(lo_ref[here], back, TN)
        out_ref[...] = (base_ref[...].astype(f32) + total).astype(out_ref.dtype)


def add_kernel(a_ref, b_ref, out_ref):
    out_ref[...] = (a_ref[...] + b_ref[...].astype(f32)).astype(out_ref.dtype)


HBM = pl.BlockSpec(memory_space=pltpu.HBM)
SMEM = pl.BlockSpec(memory_space=pltpu.SMEM)
VMEM = pl.BlockSpec(memory_space=pltpu.VMEM)
KEPT = pl.BlockSpec(memory_space=pltpu.VMEM)
FIXED = ((HBM, pltpu.HBM), (KEPT, pltpu.VMEM))


def call(kernel, ins, outs, scratch=(), mib=16):
    def fixed(spec):
        return next((space for known, space in FIXED if known is spec), None)

    run = pl.pallas_call(
        kernel,
        in_specs=ins,
        out_specs=[spec for spec, _ in outs],
        out_shape=[
            fixed(spec)(shape.shape, shape.dtype) if fixed(spec) else shape for spec, shape in outs
        ],
        scratch_shapes=list(scratch),
        compiler_params=pltpu.CompilerParams(vmem_limit_bytes=mib * 1024 * 1024),
    )

    def placed(*args):
        return run(
            *(
                pltpu.with_memory_space_constraint(arg, fixed(spec)) if fixed(spec) else arg
                for spec, arg in zip(ins, args)
            )
        )

    return placed


def body(
    query,
    forget_logit,
    value,
    out_gate,
    lower_bound,
    head_gain,
    residual_in,
    w_out,
    ffn_gain,
    routing,
    route_weight,
    expert_gate,
    expert_up,
    expert_down,
):
    shape = jax.ShapeDtypeStruct
    dma = pltpu.SemaphoreType.DMA
    ranks = lax.axis_size("sp")
    sides = lax.axis_size("tp")
    length, channels = query.shape
    part = channels // GROUP
    carried = part + part // HEAD_DIM * TAIL
    groups = ranks // GROUP
    half = length // sides
    width = w_out.shape[1]
    top = routing.shape[1]
    capacity = 2 * half * top // ranks
    slots = ranks * capacity
    units = expert_gate.shape[2]
    rank = lax.axis_index("sp")
    place = (rank * 2 + lax.axis_index("tp")).reshape(1)
    swap = [(i, i ^ 1) for i in range(sides)]

    def away(x, k):
        return lax.ppermute(x, "sp", [(i, i ^ k) for i in range(ranks)])

    weights = (expert_gate[0], expert_up[0], expert_down[0])
    *states, total, key_gate = call(
        first_kernel,
        [SMEM] + [HBM] * 3,
        [(VMEM, shape((carried, HEAD_DIM), bf16))] * GROUP
        + [(VMEM, shape((GROUP, length, part), f32))] * 2,
        [pltpu.VMEM((GROUP, length, part), bf16)] * 2
        + [pltpu.VMEM((GROUP, 1, part), f32), dma((3 * GROUP,))],
    )(place, forget_logit, value, lower_bound.reshape(1, -1))
    states = states[:1] + [away(states[k], k) for k in range(1, GROUP)]
    others = tuple(lax.ppermute(w, "tp", swap) for w in weights)
    route, weight = routing.T, route_weight.T
    other_route = lax.ppermute(route, "tp", swap)
    other_weight = lax.ppermute(weight, "tp", swap)
    other_residual = lax.ppermute(residual_in, "tp", swap)
    gated, residual, norm_gain, down_kept = call(
        gate_kernel,
        [SMEM] + [HBM] * 5,
        [
            (VMEM, shape((GROUP, length, part), f32)),
            (KEPT, shape((half, width), bf16)),
            (KEPT, shape((1, width), f32)),
            (KEPT, shape((units, width), bf16)),
        ],
        [
            pltpu.VMEM((GROUP, length, part), bf16),
            pltpu.VMEM((GROUP, 1, part), f32),
            dma((2 * GROUP + 3,)),
        ],
    )(place, out_gate, head_gain.reshape(1, -1), residual_in, ffn_gain.reshape(1, -1), weights[2])
    (totals,) = call(
        total_kernel,
        [SMEM] + [VMEM] * GROUP,
        [(VMEM, shape((carried, HEAD_DIM), bf16))],
        [pltpu.VMEM((GROUP, carried, HEAD_DIM), bf16)],
    )(place, *states)
    totals = [totals] + [away(totals, GROUP * k) for k in range(1, groups)]
    intra, qe, w_own, w_other = call(
        intra_kernel,
        [SMEM] + [VMEM] * 2 + [HBM] * 3,
        [
            (VMEM, shape((GROUP, length, part), f32)),
            (VMEM, shape((GROUP, length, part), bf16)),
            (KEPT, shape((channels, width), bf16)),
            (KEPT, shape((channels, width), bf16)),
        ],
        [pltpu.VMEM((GROUP, length, part), bf16)] * 2 + [dma((2 * GROUP + 2,))],
    )(place, total, key_gate, query, value, w_out)
    priors = call(
        functools.partial(carry_kernel, groups=groups),
        [SMEM] + [VMEM] * (GROUP + groups),
        [(VMEM, shape((part, HEAD_DIM), bf16))] * GROUP,
        [
            pltpu.VMEM((GROUP, carried, HEAD_DIM), bf16),
            pltpu.VMEM((groups, carried, HEAD_DIM), bf16),
            pltpu.VMEM((GROUP, part, HEAD_DIM), bf16),
        ],
    )(place, *states, *totals)
    priors = list(priors[:1]) + [away(priors[k], k) for k in range(1, GROUP)]

    gate_kept, up_kept = call(
        bring_kernel, [HBM] * 2, [(KEPT, shape((width, units), bf16))] * 2, [dma((2,))]
    )(*weights[:2])

    direct = capacity % 16 == 0
    box = (VMEM, shape((slots, width), bf16))
    table = (VMEM, shape((slots, half), bf16))
    tables = []
    if direct:
        *tables, hi, lo, other_hi, other_lo = call(
            functools.partial(pair_kernel, capacity=capacity), [SMEM] + [VMEM] * 4, [table] * 6
        )(place, route, weight, other_route, other_weight)

    (mixed,) = call(
        mix_kernel, [SMEM] + [VMEM] * (3 + GROUP), [(VMEM, shape((length, channels), bf16))]
    )(place, intra, qe, gated, *priors)
    recv = lax.ppermute(mixed, "tp", swap)
    (partial,) = call(
        keep_kernel, [VMEM, KEPT], [(VMEM, shape((length, width), f32))]
    )(mixed, w_own)
    recv, others = lax.optimization_barrier((recv, others))
    blocks = ranks // 2
    normed = shape((half, width), bf16)
    block = shape((2 * capacity, width), bf16)
    updated, *boxes = call(
        functools.partial(project_kernel, count=len(tables)),
        [SMEM] + [VMEM] * 2 + [KEPT] * 2 + [VMEM, KEPT] + [VMEM] * len(tables),
        [(VMEM, normed)] + ([(VMEM, block)] * blocks if direct else [(VMEM, normed)]),
        [pltpu.VMEM((length, width), f32)],
    )(place, recv, partial, w_other, residual, other_residual, norm_gain, *tables)
    kept = (gate_kept, up_kept, down_kept, *others)

    def experts(arrays):
        rows = sum(x.shape[0] for x in arrays)
        return call(
            expert_kernel,
            [VMEM] * len(arrays) + [KEPT] * 6,
            [(VMEM, shape(x.shape, bf16)) for x in arrays],
            [pltpu.VMEM((rows, width), bf16), pltpu.VMEM((rows, 2 * units), bf16)],
        )(*arrays, *kept)

    def combine(sums, arrays, start, kind):
        rows = sum(x.shape[0] for x in arrays)
        return call(
            functools.partial(combine_kernel, start=start, count=len(sums)),
            [VMEM] * (3 * len(sums) + len(arrays)),
            [(VMEM, shape((half, width), kind))] * len(sums),
            [pltpu.VMEM((rows, width), bf16)],
        )(*(x for entry in sums for x in entry), *arrays)

    if not direct:

        def exchange(x):
            order = jnp.arange(ranks, dtype=jnp.int32) ^ rank
            x = jnp.take(x.reshape(ranks, capacity, width), order, axis=0)
            x = lax.all_to_all(x, "sp", split_axis=0, concat_axis=0, tiled=True)
            return jnp.take(x, order, axis=0).reshape(slots, width)

        outbox, hi, lo = call(
            functools.partial(own_kernel, capacity=capacity),
            [SMEM] + [VMEM] * 3,
            [box, table, table],
        )(place, route, weight, *boxes)
        (result,) = experts([exchange(outbox)])
        return combine([(updated, hi, lo)], [exchange(result)], 0, bf16)[0]

    def paired(x, j):
        pairs = [
            (i * sides + side, (i ^ (2 * j + side)) * sides + side)
            for i in range(ranks)
            for side in range(sides)
        ]
        return lax.ppermute(x, ("sp", "tp"), pairs)

    near = list(range(blocks // 2))
    early = list(range(blocks // 2, blocks * 3 // 4))
    late = list(range(blocks * 3 // 4, blocks))
    arrived = [paired(x, j) for j, x in enumerate(boxes)]
    back = [None] * blocks
    for group in (early, near, late):
        for j, x in zip(group, experts([arrived[j] for j in group])):
            back[j] = paired(x, j)
    zero = jnp.zeros((half, width), bf16)
    own, other = combine(
        [(updated, hi, lo), (zero, other_hi, other_lo)], [back[j] for j in near], 0, f32
    )
    start = len(near) * 2 * capacity
    rest = [back[j] for j in early + late]
    (other,) = combine([(other, other_hi, other_lo)], rest, start, bf16)
    extra = lax.ppermute(other, "tp", swap)
    (own,) = combine([(own, hi, lo)], rest, start, f32)
    (layer_out,) = call(add_kernel, [VMEM] * 2, [(VMEM, shape((half, width), bf16))])(own, extra)
    return layer_out


def solution(mesh):
    placed = (
        P("sp", "tp"),
        P("sp", "tp"),
        P("sp", "tp"),
        P("sp", "tp"),
        P("tp"),
        P("tp"),
        P(("sp", "tp"), None),
        P(),
        P(),
        P(("sp", "tp"), None),
        P(("sp", "tp"), None),
        P("sp", None, "tp"),
        P("sp", None, "tp"),
        P("sp", "tp", None),
    )

    return jax.shard_map(
        body, mesh=mesh, in_specs=placed, out_specs=P(("sp", "tp"), None), check_vma=False
    )
```
